256 devices in a mesh: ep: 64 (over z, y, core), tp: 4 (over x).
Axes of the slice: x: 4, y: 4, z: 8, core: 2. Of those that a mesh axis runs over, the one named last changes fastest.
Arguments:
- q_heads: bfloat16 [65536, 1024], P('ep', 'tp'), may hold values from -200 to 200
- k_heads: bfloat16 [65536, 256], P('ep', 'tp'), may hold values from -6 to 6
- v_heads: bfloat16 [65536, 256], P('ep', 'tp'), may hold values from -6 to 6
- sink_logits: float32 [16], P('tp'), may hold values from 1 to 5
- out_weight: bfloat16 [1024, 2048], P(None, 'tp'), may hold values from -1.5 to 1.5
- tokens_b: bfloat16 [32768, 2048], P('ep'), may hold values from -6 to 6
- moe_gain: float32 [2048], replicated, may hold values from 0.1 to 1.9
- router_group: bfloat16 [2048, 4], replicated, may hold values from -0.125 to 0.125
- router_expert: bfloat16 [2048, 128], replicated, may hold values from -0.125 to 0.125
- route_expert: int32 [32768, 2], P('ep'), may hold values from 0 to 127, as said below
- expert_gate: bfloat16 [128, 2048, 1024], P('ep', None, 'tp'), may hold values from -0.125 to 0.125
- expert_up: bfloat16 [128, 2048, 1024], P('ep', None, 'tp'), may hold values from -0.125 to 0.125
- expert_down: bfloat16 [128, 1024, 2048], P('ep', 'tp'), may hold values from -0.75 to 0.75
Outputs:
- mixer_out: bfloat16 [65536, 2048], P('ep', 'tp')
- moe_out: bfloat16 [32768, 2048], P(('ep', 'tp'))
The draws below stay inside these ranges and needn't reach their ends.
Inputs may be any that keep to these rules, and one draw needn't show every extreme that they name: `route_expert`: each token names two different experts, in rising order, of one group of 32 consecutive experts. In each aligned block of 128 rows (the rows of one device) no expert is named by more than 4 tokens, in each group one expert is named by exactly 4 tokens of every block, and each group is named by a quarter of every block's tokens.
All inputs are finite; a program needn't handle non-finite values.
Results may differ from the reference program's by a relative error of at most 0.011.
Values may be sent and summed in bfloat16 or wider, within the bound.
A program may use at most 128 MiB of HBM per device.

```python
import jax
import jax.numpy as jnp
from jax import lax

D = 2048
HEADS = 16
KV = 4
HD = 64
WINDOW = 128
ROW_B = 128
GROUPS = 4
FF = 1024
EXPERTS = 128
GROUP_EXPERTS = 32
CAP = 4
TOK_A = 65536
TOK_B = 32768
N_EP = 64
N_TP = 4


def pair_heads(seed_key):
    key_query, key_keys = jax.random.split(seed_key, 2)
    group_size = HEADS // KV
    queries = jnp.clip(jax.random.normal(key_query, (TOK_A, KV, group_size, HD), jnp.float32), -5.0, 5.0)
    keys_raw = jnp.clip(jax.random.normal(key_keys, (TOK_A, KV, HD), jnp.float32), -5.0, 5.0)
    return (queries.reshape(TOK_A, HEADS * HD), keys_raw.reshape(TOK_A, KV * HD))


def draw_q_heads(key, part):
    return pair_heads(jax.random.fold_in(key, 3))[0].astype(jnp.bfloat16)


def draw_k_heads(key, part):
    return pair_heads(jax.random.fold_in(key, 3))[1].astype(jnp.bfloat16)


def draw_route_expert(key, part):
    block_count = N_EP * N_TP
    half_rows = ROW_B // 2
    quarter_rows = ROW_B // 4
    pool = jnp.repeat(jnp.arange(GROUP_EXPERTS, dtype=jnp.int32), CAP)
    favored = jax.random.randint(jax.random.fold_in(key, 7), (GROUPS,), 0, GROUP_EXPERTS)

    def one_group(group_key, group_index):
        ranks = jax.random.permutation(group_key, pool.shape[0]).astype(jnp.int32)
        ordering = jnp.where(pool == favored[group_index], -1, ranks)
        order = jnp.argsort(ordering, stable=True)
        picked = jnp.sort(pool[order[:half_rows]])
        pairs = jnp.stack([picked[:quarter_rows], picked[quarter_rows:]], axis=1)
        return pairs + group_index * GROUP_EXPERTS

    def one_block(block_key):
        group_keys = jax.random.split(block_key, GROUPS + 1)
        pairs = jax.vmap(one_group)(group_keys[:GROUPS], jnp.arange(GROUPS, dtype=jnp.int32))
        pairs = pairs.reshape(ROW_B, 2)
        return pairs[jax.random.permutation(group_keys[GROUPS], ROW_B)]
    block_keys = jax.random.split(jax.random.fold_in(key, 11), block_count)
    return jax.vmap(one_block)(block_keys).reshape(block_count * ROW_B, 2).astype(jnp.int32)


def block_levels(own_key, dims, cuts, low, largest):
    loudness, own = 1.0, jax.random.fold_in(own_key, 6)
    for axis_at, shards_of in cuts:
        heights = jnp.exp(jax.random.uniform(jax.random.fold_in(own, axis_at), (shards_of,), jnp.float32, low / len(cuts), largest / len(cuts)))
        loudness = loudness * jnp.repeat(heights, dims[axis_at] // shards_of).reshape([-1 if axis == axis_at else 1 for axis in range(len(dims))])
    return loudness


def scatter_about(key, dims, spread, limit, cuts=(), held_as=jnp.bfloat16):
    result = spread * jax.random.normal(key, dims, jnp.float32)
    if cuts:
        result = result * block_levels(key, dims, cuts, -0.22, 0.18)
    return jnp.clip(result, -limit, limit).astype(held_as)


def setup_inputs(seed: int = 0) -> dict:
    key_of = jax.random.split(jax.random.key(seed), 14)
    q_heads = draw_q_heads(jax.random.fold_in(key_of[13], 71), 0)
    k_heads = draw_k_heads(jax.random.fold_in(key_of[13], 71), 0)
    v_heads = scatter_about(key_of[2], (TOK_A, KV * HD), 1.0, 6.0, ((0, 64), (1, 4)))
    sink_logits = jnp.clip(1.0 + 4.0 * jax.random.uniform(key_of[3], (HEADS,), jnp.float32) ** block_levels(key_of[3], (HEADS,), ((0, 4),), -0.2, 0.2), 1.0, 5.0)
    out_weight = scatter_about(key_of[4], (HEADS * HD, D), HEADS ** -0.5, 1.5, ((1, 4),))
    tokens_b = scatter_about(key_of[5], (TOK_B, D), 1.0, 6.0, ((0, 64),))
    moe_gain = jnp.clip(1.0 + 0.18 * jax.random.normal(key_of[6], (D,), jnp.float32), 0.1, 1.9)
    router_group = scatter_about(key_of[7], (D, GROUPS), D ** -0.5, 0.125)
    router_expert = scatter_about(key_of[8], (D, EXPERTS), D ** -0.5, 0.125)
    route_expert = draw_route_expert(jax.random.fold_in(key_of[13], 71), 0)
    expert_gate = scatter_about(key_of[10], (EXPERTS, D, FF), D ** -0.5, 0.125, ((0, 64), (2, 4)))
    expert_up = scatter_about(key_of[11], (EXPERTS, D, FF), D ** -0.5, 0.125, ((0, 64), (2, 4)))
    expert_down = scatter_about(key_of[12], (EXPERTS, FF, D), (FF // 16) ** -0.5, 0.75, ((0, 64), (1, 4)))
    return {"q_heads": q_heads, "k_heads": k_heads, "v_heads": v_heads, "sink_logits": sink_logits, "out_weight": out_weight, "tokens_b": tokens_b, "moe_gain": moe_gain, "router_group": router_group, "router_expert": router_expert, "route_expert": route_expert, "expert_gate": expert_gate, "expert_up": expert_up, "expert_down": expert_down}


def banded(values, blocks, span_len):
    shaped = values.reshape(TOK_A, KV, HD)
    padded = jnp.concatenate([jnp.zeros((span_len, KV, HD), shaped.dtype), shaped], axis=0)
    padded = padded.reshape(blocks + 1, span_len, KV, HD)
    band = jnp.concatenate([padded[:-1], padded[1:]], axis=1)
    return jnp.moveaxis(band, 2, 0)

def gate_weights(normed, routes, router_group, router_expert):
    group_logits = jnp.dot(normed, router_group, preferred_element_type=jnp.float32)
    expert_logits = jnp.dot(normed, router_expert, preferred_element_type=jnp.float32)
    group_count = router_group.shape[1]
    expert_count = router_expert.shape[1]
    chosen_group = routes[:, 0] // (expert_count // group_count)
    group_match = chosen_group[:, None] == jnp.arange(group_count, dtype=jnp.int32)[None, :]
    group_share = lax.optimization_barrier(jnp.sum(jnp.where(group_match, jax.nn.softmax(group_logits, axis=-1), 0.0), axis=-1))
    expert_match = routes[:, :, None] == jnp.arange(expert_count, dtype=jnp.int32)[None, None, :]
    picked = lax.optimization_barrier(jnp.sum(jnp.where(expert_match, expert_logits[:, None, :], 0.0), axis=-1))
    return group_share[:, None] * jax.nn.softmax(picked, axis=-1)

def reference(q_heads, k_heads, v_heads, sink_logits, out_weight, tokens_b, moe_gain, router_group, router_expert, route_expert, expert_gate, expert_up, expert_down):
    span_len = WINDOW
    blocks = TOK_A // span_len
    group_size = HEADS // KV
    query_blocks = jnp.moveaxis(q_heads.reshape(blocks, span_len, KV, group_size, HD), 2, 0)
    key_band = banded(k_heads, blocks, span_len)
    value_band = banded(v_heads, blocks, span_len)
    query_index = jnp.arange(span_len, dtype=jnp.int32)[:, None]
    key_index = jnp.arange(2 * span_len, dtype=jnp.int32)[None, :]
    distance = query_index + span_len - key_index
    key_place = jnp.arange(blocks, dtype=jnp.int32)[:, None, None] * span_len + key_index[None] - span_len
    allowed = (distance >= 0)[None] & (distance < span_len)[None] & (key_place >= 0)
    sink_rows = sink_logits.reshape(KV, group_size)

    def one_head(packed):
        query_block, key_rows, value_rows, sink_row = packed
        scores = jnp.einsum('nqgd,nkd->ngqk', query_block.astype(jnp.float32), key_rows.astype(jnp.float32)) * HD ** (-0.5)
        masked = jnp.where(allowed[:, None], scores, -1e+30)
        sink_full = sink_row[None, :, None]
        row_max = jnp.maximum(lax.optimization_barrier(jnp.max(masked, axis=-1)), sink_full)
        weights_exp = jnp.exp(masked - row_max[..., None])
        denominator = lax.optimization_barrier(jnp.sum(weights_exp, axis=-1)) + jnp.exp(sink_full - row_max)
        probs = lax.optimization_barrier((weights_exp / denominator[..., None]).astype(jnp.bfloat16))
        mixed = jnp.einsum('ngqk,nkd->nqgd', probs.astype(jnp.float32), value_rows.astype(jnp.float32))
        return mixed.astype(jnp.bfloat16)
    attended = lax.map(one_head, (query_blocks, key_band, value_band, sink_rows))
    attended = jnp.moveaxis(attended, 0, 2).reshape(TOK_A, HEADS * HD)
    mixer_out = jnp.dot(attended, out_weight, preferred_element_type=jnp.float32).astype(jnp.bfloat16)
    blocks_b = N_EP * N_TP
    values = tokens_b.astype(jnp.float32)
    normed = (values * lax.rsqrt(lax.optimization_barrier(jnp.mean(values * values, axis=-1, keepdims=True)) + 1e-06) * moe_gain).astype(jnp.bfloat16)
    gates = gate_weights(normed, route_expert, router_group, router_expert)
    flat_routes = route_expert.reshape(blocks_b, 2 * ROW_B)
    onehot = (flat_routes[:, :, None] == jnp.arange(EXPERTS, dtype=jnp.int32)[None, None, :]).astype(jnp.int32)
    places = lax.optimization_barrier(jnp.sum(onehot * jnp.cumsum(onehot, axis=1), axis=2)) - 1
    token_ids = (jnp.arange(TOK_B * 2, dtype=jnp.int32) // 2).reshape(blocks_b, 2 * ROW_B)
    block_ids = jnp.broadcast_to(jnp.arange(blocks_b, dtype=jnp.int32)[:, None], (blocks_b, 2 * ROW_B))
    slot_token = jnp.full((EXPERTS, blocks_b, CAP), TOK_B, jnp.int32).at[flat_routes, block_ids, places].set(token_ids)
    slot_gate = jnp.zeros((EXPERTS, blocks_b, CAP), jnp.float32).at[flat_routes, block_ids, places].set(gates.reshape(blocks_b, 2 * ROW_B))
    padded_rows = jnp.concatenate([normed, jnp.zeros((1, D), jnp.bfloat16)], axis=0)
    hidden_block = FF // N_TP

    def one_expert(running, packed):
        token_list, gate_list, w_gate, w_up, w_down = packed
        rows_in = padded_rows[token_list]
        gate_pre = jnp.dot(rows_in, w_gate, preferred_element_type=jnp.float32)
        up_pre = jnp.dot(rows_in, w_up, preferred_element_type=jnp.float32)
        activated = lax.optimization_barrier((jax.nn.silu(gate_pre) * up_pre).astype(jnp.bfloat16))
        pieces = jnp.einsum('ntf,tfd->ntd', activated.reshape(-1, N_TP, hidden_block).astype(jnp.float32), w_down.reshape(N_TP, hidden_block, D).astype(jnp.float32))
        pieces = lax.optimization_barrier(pieces.astype(jnp.bfloat16)).astype(jnp.float32)
        expert_out = lax.optimization_barrier(lax.optimization_barrier(jnp.sum(pieces, axis=1)).astype(jnp.bfloat16)).astype(jnp.float32)
        running = running.at[token_list].add(gate_list[:, None] * expert_out)
        return (running, None)
    running = jnp.zeros((TOK_B + 1, D), jnp.float32)
    running, _ = lax.scan(one_expert, running, (slot_token.reshape(EXPERTS, -1), slot_gate.reshape(EXPERTS, -1), expert_gate, expert_up, expert_down))
    moe_out = running[:TOK_B].astype(jnp.bfloat16)
    return (mixer_out, moe_out)
```

```python
import functools

import jax
import jax.numpy as jnp
from jax import lax
from jax.experimental import pallas as pl
from jax.experimental.pallas import tpu as pltpu
from jax.sharding import PartitionSpec as P

HEADS = 16
KV = 4
HD = 64
WINDOW = 128
CAP = 4
GROUPS = 4
NTP = 4
PLANE = 8
MESH = pl.DeviceIdType.MESH
F32 = jnp.float32
BF16 = jnp.bfloat16


def shifted(value, axis, steps):
    count = lax.axis_size(axis)
    leading, last = (max(0, -steps), min(count, count - steps))
    return lax.ppermute(value, axis, [(source, source + steps) for source in range(leading, last)])


def hop_of(i, nz):
    if i == 0:
        return 0
    return (nz - i) // 2 if i % 2 == 0 else (i + nz - 1) // 2


def position_of(d, nz):
    return jnp.where(d == 0, 0, jnp.where(d < nz // 2, nz - 2 * d, 2 * d - nz + 1))


def slot_rows(expert, block, place, z, yc, nz, nyc):
    rank = expert >> 1
    d = lax.rem(lax.div(rank, nyc) - z + nz, nz)
    j = lax.rem(lax.rem(rank, nyc) - yc + nyc, nyc)
    return ((position_of(d, nz) * nyc + j) * 2 + (expert & 1)) * (NTP * CAP) + block * CAP + place


def prep_kernel(nz, nyc, tok, gain, routes_t, routes, r_group, r_expert, slots, gates, rows_out, normed):
    x = lax.axis_index("tp")
    e = lax.axis_index("ep")
    z, yc = lax.div(e, nyc), lax.rem(e, nyc)
    tokens, width = tok.shape
    block_rows = tokens // NTP
    experts = r_expert.shape[1]
    fq = width // NTP
    step = tokens // 8

    def norm_rows(i, carry):
        rows = pl.ds(pl.multiple_of(i * step, step), step)
        v = tok[rows, :].astype(F32)
        ms = jnp.mean(v * v, axis=-1, keepdims=True)
        normed[rows, :] = (v * lax.rsqrt(ms + 1e-06) * gain[...]).astype(BF16)
        return carry

    lax.fori_loop(0, 8, norm_rows, 0)

    def iota(shape, dim):
        return lax.broadcasted_iota(jnp.int32, shape, dim)

    first, second = (iota((tokens, tokens), 0), iota((tokens, tokens), 1))
    same = lax.div(first, block_rows) == lax.div(second, block_rows)
    e0, e1 = routes_t[0:1, :], routes_t[1:2, :]
    ids = iota((experts, tokens), 0)
    hit0, hit1 = ids == e0, ids == e1
    before = jnp.where(same & (first < second), 1.0, 0.0).astype(BF16)
    both = jnp.where(hit0 | hit1, 1.0, 0.0).astype(BF16)
    count = jnp.dot(both, before, preferred_element_type=F32)
    place0 = jnp.sum(jnp.where(hit0, count, 0.0), axis=0, keepdims=True).astype(jnp.int32)
    place1 = jnp.sum(jnp.where(hit1, count, 0.0), axis=0, keepdims=True).astype(jnp.int32)
    block = lax.div(iota((1, tokens), 1), block_rows)
    t0 = slot_rows(e0, block, place0, z, yc, nz, nyc)
    t1 = slot_rows(e1, block, place1, z, yc, nz, nyc)
    part = nyc * 2 * NTP * CAP
    mine = normed[:, pl.ds(pl.multiple_of(x * fq, fq), fq)]

    def fill(i, carry):
        ids = iota((part, tokens), 0) + i * part
        pick = jnp.where((ids == t0) | (ids == t1), 1.0, 0.0).astype(BF16)
        got = jnp.dot(pick, mine, preferred_element_type=F32).astype(BF16)
        slots[i] = got.reshape(nyc, 2, NTP * CAP, fq)
        return carry

    lax.fori_loop(0, nz, fill, 0)
    c0, c1 = routes[:, 0:1], routes[:, 1:2]
    ids = iota((tokens, experts), 1)
    hit0, hit1 = ids == c0, ids == c1
    after = jnp.where(same & (second < first), 1.0, 0.0).astype(BF16)
    both = jnp.where(hit0 | hit1, 1.0, 0.0).astype(BF16)
    count = jnp.dot(after, both, preferred_element_type=F32)
    place0 = jnp.sum(jnp.where(hit0, count, 0.0), axis=1, keepdims=True).astype(jnp.int32)
    place1 = jnp.sum(jnp.where(hit1, count, 0.0), axis=1, keepdims=True).astype(jnp.int32)
    block = lax.div(iota((tokens, 1), 0), block_rows)
    rows_out[:, 0:1] = slot_rows(c0, block, place0, z, yc, nz, nyc)
    rows_out[:, 1:2] = slot_rows(c1, block, place1, z, yc, nz, nyc)
    by_expert = jnp.dot(normed[...], r_expert[...], preferred_element_type=F32)
    by_group = jnp.dot(normed[...], r_group[...], preferred_element_type=F32)
    groups = r_group.shape[1]
    group_max = jnp.max(by_group, axis=1, keepdims=True)
    group_exp = jnp.exp(by_group - group_max)
    chosen = iota((tokens, groups), 1) == lax.div(c0, experts // groups)
    share = jnp.sum(jnp.where(chosen, group_exp, 0.0), axis=1, keepdims=True) / jnp.sum(
        group_exp, axis=1, keepdims=True
    )
    l0 = jnp.sum(jnp.where(hit0, by_expert, 0.0), axis=1, keepdims=True)
    l1 = jnp.sum(jnp.where(hit1, by_expert, 0.0), axis=1, keepdims=True)
    top = jnp.maximum(l0, l1)
    x0, x1 = jnp.exp(l0 - top), jnp.exp(l1 - top)
    gates[:, 0:1] = share * (x0 / (x0 + x1))
    gates[:, 1:2] = share * (x1 / (x0 + x1))


def moe_kernel(
    nz, nyc, s_hbm, wg_hbm, wu_hbm, wd_hbm, att_hbm, ow_hbm, gates, rows_in, mix, moe,
    relay, arr, wg, wu, wq, act, out, back, ret, att, ow, fin_out, fin,
    zs, zr, ys, yr, xs, xr, fs, fr, acs, acr, afs, afr, ws, wr,
    rzs, rzr, rys, ryr, ts, tr, tfs, tfr, es, er, loc,
):
    x = lax.axis_index("tp")
    e = lax.axis_index("ep")
    z, yc = lax.div(e, nyc), lax.rem(e, nyc)
    fq = arr.shape[-1]
    hq = wg.shape[-1]
    hops = [hop_of(i, nz) for i in range(nz)]
    half = nyc // 2
    pairs = nz // 2

    def zdev(d):
        return (lax.rem(z + (d + nz), nz) * nyc + yc, x)

    def ydev(j):
        return (z * nyc + lax.rem(yc + (j + nyc), nyc), x)

    def xdev(q):
        return (e, lax.rem(x + q, NTP))

    def column(q):
        return lax.rem(x + q, NTP)

    def send(src, dst, s_sem, r_sem, dev):
        copy = pltpu.make_async_remote_copy(
            src_ref=src, dst_ref=dst, send_sem=s_sem, recv_sem=r_sem,
            device_id=dev, device_id_type=MESH,
        )
        copy.start()

    def drain(ref, sem):
        pltpu.make_async_copy(ref, ref, sem).wait()

    barrier = pltpu.get_barrier_semaphore()
    peers = [zdev(d) for d in range(1, nz)] + [ydev(j) for j in range(1, nyc)]
    peers += [xdev(q) for q in range(1, NTP)]
    for peer in peers:
        pl.semaphore_signal(barrier, inc=1, device_id=peer, device_id_type=MESH)
    local = [
        pltpu.make_async_copy(s_hbm.at[0, 0], arr.at[0, 0, 0], loc.at[0]),
        pltpu.make_async_copy(wg_hbm, wg, loc.at[1]),
        pltpu.make_async_copy(wu_hbm, wu, loc.at[2]),
        pltpu.make_async_copy(
            wd_hbm.at[:, :, pl.ds(pl.multiple_of(x * fq, fq), fq)], wq.at[0], loc.at[3]
        ),
        pltpu.make_async_copy(att_hbm, att.at[0], loc.at[4]),
        pltpu.make_async_copy(ow_hbm, ow, loc.at[5]),
    ]
    for copy in local:
        copy.start()
    pl.semaphore_wait(barrier, len(peers))

    for i in range(1, nz):
        send(s_hbm.at[i, 0], arr.at[0, i, 0], zs.at[i, 0], zr.at[i, 0], zdev(hops[i]))
        send(
            s_hbm.at[i, pl.ds(1, nyc - 1)], relay.at[i, pl.ds(1, nyc - 1)],
            zs.at[i, 1], zr.at[i, 1], zdev(hops[i]),
        )
    for j in range(1, nyc):
        send(s_hbm.at[0, j], arr.at[0, 0, j], ys.at[0], yr.at[0], ydev(j))
    for q in range(1, NTP):
        cols = pl.ds(pl.multiple_of(column(q) * fq, fq), fq)
        send(wd_hbm.at[:, :, cols], wq.at[q], ws.at[q], wr.at[q], xdev(q))

    def plane_out(i):
        if i == 0:
            return
        drain(relay.at[i, pl.ds(1, nyc - 1)], zr.at[i, 1])
        for j in range(1, nyc):
            send(relay.at[i, j], arr.at[0, i, j], ys.at[i], yr.at[i], ydev(j))

    def ring_own(i):
        if i == 0:
            local[0].wait()
        else:
            drain(arr.at[0, i, 0], zr.at[i, 0])
        drain(arr.at[0, i, pl.ds(1, nyc - 1)], yr.at[i])
        send(arr.at[0, i], arr.at[1, i], xs.at[i, 0], xr.at[i, 0], xdev(1))
        send(arr.at[0, i], arr.at[3, i], xs.at[i, 1], xr.at[i, 1], xdev(3))

    def ring_on(i):
        low, high = pl.ds(0, half), pl.ds(half, half)
        drain(arr.at[1, i], xr.at[i, 0])
        send(arr.at[1, i, low], arr.at[2, i, low], fs.at[i, 0], fr.at[i, 0], xdev(1))
        drain(arr.at[3, i], xr.at[i, 1])
        send(arr.at[3, i, high], arr.at[2, i, high], fs.at[i, 1], fr.at[i, 1], xdev(3))

    def ring_in(i):
        drain(arr.at[2, i, pl.ds(0, half)], fr.at[i, 0])
        drain(arr.at[2, i, pl.ds(half, half)], fr.at[i, 1])

    rows2 = 2 * nyc * NTP * CAP

    def hidden(p):
        if p == 0:
            local[1].wait()
            local[2].wait()

        def one(k, carry):
            gate = jnp.zeros((rows2, hq), F32)
            up = jnp.zeros((rows2, hq), F32)
            for q in range(NTP):
                depth = pl.ds(pl.multiple_of(column(NTP - q) * fq, fq), fq)
                rows = arr[q, pl.ds(2 * p, 2), :, k].reshape(rows2, fq)
                gate += jnp.dot(rows, wg[k, depth, :], preferred_element_type=F32)
                up += jnp.dot(rows, wu[k, depth, :], preferred_element_type=F32)
            value = (gate / (1.0 + jnp.exp(-gate)) * up).astype(BF16)
            act[0, p, k] = value
            return carry

        lax.fori_loop(0, 2, one, 0)
        send(act.at[0, p], act.at[1, p], acs.at[p, 0], acr.at[p, 0], xdev(1))
        send(act.at[0, p], act.at[3, p], acs.at[p, 1], acr.at[p, 1], xdev(3))

    def act_on(p):
        drain(act.at[1, p], acr.at[p, 0])
        send(act.at[1, p, 0], act.at[2, p, 0], afs.at[p, 0], afr.at[p, 0], xdev(1))
        drain(act.at[3, p], acr.at[p, 1])
        send(act.at[3, p, 1], act.at[2, p, 1], afs.at[p, 1], afr.at[p, 1], xdev(3))

    def down(p):
        if p == 0:
            local[3].wait()
            for q in range(1, NTP):
                drain(wq.at[q], wr.at[q])
        drain(act.at[2, p, 0], afr.at[p, 0])
        drain(act.at[2, p, 1], afr.at[p, 1])

        def one(k, carry):
            total = jnp.zeros((rows2, fq), F32)
            for q in range(NTP):
                total += jnp.dot(act[q, p, k], wq[q, k], preferred_element_type=F32)
            out[pl.ds(2 * p, 2), :, k] = total.astype(BF16).reshape(2, nyc, NTP * CAP, fq)
            return carry

        lax.fori_loop(0, 2, one, 0)
        for i in (2 * p, 2 * p + 1):
            if i == 0:
                ret[0, 0] = out[0, 0]
                for j in range(1, nyc):
                    send(out.at[0, j], ret.at[0, j], rys.at[0], ryr.at[0], ydev(-j))
                continue
            rest = pl.ds(1, nyc - 1)
            send(out.at[i, rest], back.at[i, rest], rzs.at[i, 1], rzr.at[i, 1], zdev(-hops[i]))
            send(out.at[i, 0], ret.at[i, 0], rzs.at[i, 0], rzr.at[i, 0], zdev(-hops[i]))

    def plane_back(i):
        if i == 0:
            return
        drain(back.at[i, pl.ds(1, nyc - 1)], rzr.at[i, 1])
        for j in range(1, nyc):
            send(back.at[i, j], ret.at[i, j], rys.at[i], ryr.at[i], ydev(-j))

    for n in range(nz + 2):
        if n < nz:
            plane_out(n)
        if 0 <= n - 1 < nz:
            ring_own(n - 1)
        if 0 <= n - 2 < nz:
            ring_on(n - 2)
        m = n - 3
        if m >= 0:
            ring_in(m)
            if m % 2 == 1:
                hidden(m // 2)
                if m >= 3:
                    down(m // 2 - 1)
            elif m >= 2:
                act_on(m // 2 - 1)
    ring_in(nz - 1)
    hidden(pairs - 1)
    if pairs > 1:
        down(pairs - 2)
    act_on(pairs - 1)
    rows = att.shape[1]
    top, bottom = pl.ds(0, rows // 2), pl.ds(rows // 2, rows // 2)
    send(att_hbm, att.at[1], ts.at[0], tr.at[0], xdev(1))
    send(att_hbm, att.at[3], ts.at[1], tr.at[1], xdev(3))
    for i in range(nz - 2):
        plane_back(i)
    down(pairs - 1)
    drain(att.at[1], tr.at[0])
    send(att.at[1, top], att.at[2, top], tfs.at[0], tfr.at[0], xdev(1))
    drain(att.at[3], tr.at[1])
    send(att.at[3, bottom], att.at[2, bottom], tfs.at[1], tfr.at[1], xdev(3))
    for i in range(nz - 2, nz):
        plane_back(i)
    local[4].wait()
    local[5].wait()
    drain(att.at[2, top], tfr.at[0])
    drain(att.at[2, bottom], tfr.at[1])
    chunk = rows // 4
    hw = att.shape[2]

    def project(c, carry):
        where = pl.ds(pl.multiple_of(c * chunk, chunk), chunk)
        total = jnp.zeros((chunk, ow.shape[1]), F32)
        for q in range(NTP):
            depth = pl.ds(pl.multiple_of(column(NTP - q) * hw, hw), hw)
            total += jnp.dot(att[q, where, :], ow[depth, :], preferred_element_type=F32)
        mix[where, :] = total.astype(BF16)
        return carry

    lax.fori_loop(0, 4, project, 0)

    for i in range(nz):
        if i > 0:
            drain(ret.at[i, 0], rzr.at[i, 0])
        drain(ret.at[i, pl.ds(1, nyc - 1)], ryr.at[i])

    slots = nz * nyc * 2 * NTP * CAP
    block_rows = gates.shape[0] // NTP

    def combined(t):
        where = pl.ds(pl.multiple_of(t * block_rows, block_rows), block_rows)
        ids = lax.broadcasted_iota(jnp.int32, (block_rows, slots), 1)
        at = rows_in[where, :]
        pick = jnp.concatenate(
            [jnp.where(ids == at[:, k : k + 1], 1.0, 0.0).astype(BF16) for k in range(2)], axis=0
        )
        got = jnp.dot(pick, ret[...].reshape(slots, fq), preferred_element_type=F32)
        g = gates[where, :]
        return (g[:, 0:1] * got[:block_rows] + g[:, 1:2] * got[block_rows:]).astype(BF16)

    for q in range(1, NTP):
        fin_out[q] = combined(column(q))
        send(fin_out.at[q], fin.at[q], es.at[q], er.at[q], xdev(q))
    moe[:, pl.ds(pl.multiple_of(x * fq, fq), fq)] = combined(x)
    for q in range(1, NTP):
        drain(fin.at[q], er.at[q])
        moe[:, pl.ds(pl.multiple_of(column(NTP - q) * fq, fq), fq)] = fin[q]

    rest = pl.ds(1, nyc - 1)
    for i in range(nz):
        if i > 0:
            drain(relay.at[i, 0], zs.at[i, 0])
            drain(relay.at[i, rest], zs.at[i, 1])
            drain(out.at[i, 0], rzs.at[i, 0])
            drain(out.at[i, rest], rzs.at[i, 1])
        drain(arr.at[0, i, rest], ys.at[i])
        drain(ret.at[i, rest], rys.at[i])
        for way in range(2):
            drain(arr.at[0, i], xs.at[i, way])
            drain(arr.at[0, i, pl.ds(0, half)], fs.at[i, way])
    for p in range(pairs):
        for way in range(2):
            drain(act.at[0, p], acs.at[p, way])
            drain(act.at[0, p, 0], afs.at[p, way])
    for way in range(2):
        drain(att.at[0], ts.at[way])
        drain(att.at[0, top], tfs.at[way])
    for q in range(1, NTP):
        drain(wq.at[q], ws.at[q])
        drain(fin_out.at[q], es.at[q])


def attention(q_heads, k_heads, v_heads, sink_logits):
    span_len = WINDOW
    row_count = q_heads.shape[0]
    kv_local = k_heads.shape[1] // HD
    group_size = HEADS // KV
    blocks = row_count // span_len
    stacked = jnp.stack([k_heads[row_count - span_len :], v_heads[row_count - span_len :]])
    earlier = shifted(stacked, "ep", 1)

    def make_band(own_rows, prev_rows):
        extended = jnp.concatenate([prev_rows, own_rows], axis=0).reshape(
            blocks + 1, span_len, kv_local, HD
        )
        return jnp.concatenate([extended[:-1], extended[1:]], axis=1)

    key_band = make_band(k_heads, earlier[0])
    value_band = make_band(v_heads, earlier[1])
    query_blocks = q_heads.reshape(blocks, span_len, kv_local, group_size, HD)
    scores = jnp.einsum(
        "nqhgd,nkhd->nhgqk", query_blocks, key_band, preferred_element_type=jnp.float32
    ) * HD ** (-0.5)
    first_row = lax.axis_index("ep") * row_count
    query_index = jnp.arange(span_len, dtype=jnp.int32)[:, None]
    key_index = jnp.arange(2 * span_len, dtype=jnp.int32)[None, :]
    distance = query_index + span_len - key_index
    key_place = (
        first_row
        + jnp.arange(blocks, dtype=jnp.int32)[:, None, None] * span_len
        + key_index[None]
        - span_len
    )
    allowed = (distance >= 0)[None] & (distance < span_len)[None] & (key_place >= 0)
    masked = jnp.where(allowed[:, None, None], scores, -1e30)
    sink_full = sink_logits.reshape(kv_local, group_size)[None, :, :, None]
    row_max = jnp.maximum(jnp.max(masked, axis=-1), sink_full)
    weights_exp = jnp.exp(masked - row_max[..., None])
    denominator = jnp.sum(weights_exp, axis=-1) + jnp.exp(sink_full - row_max)
    probs = (weights_exp / denominator[..., None]).astype(jnp.bfloat16)
    attended = jnp.einsum(
        "nhgqk,nkhd->nqhgd", probs, value_band, preferred_element_type=jnp.float32
    )
    return attended.astype(jnp.bfloat16).reshape(row_count, kv_local * group_size * HD)


def per_device(
    q_heads,
    k_heads,
    v_heads,
    sink_logits,
    out_weight,
    tokens_b,
    moe_gain,
    router_group,
    router_expert,
    route_expert,
    expert_gate,
    expert_up,
    expert_down,
):
    nyc = min(PLANE, lax.axis_size("ep"))
    nz = lax.axis_size("ep") // nyc
    tokens, width = tokens_b.shape
    fq = width // NTP
    hq = expert_gate.shape[2]
    sixteen = NTP * CAP
    attended = attention(q_heads, k_heads, v_heads, sink_logits)
    vmem = pl.BlockSpec(memory_space=pltpu.VMEM)
    anywhere = pl.BlockSpec(memory_space=pl.ANY)
    slots, gates, rows = pl.pallas_call(
        functools.partial(prep_kernel, nz, nyc),
        out_shape=(
            jax.ShapeDtypeStruct((nz, nyc, 2, sixteen, fq), BF16),
            jax.ShapeDtypeStruct((tokens, 2), F32),
            jax.ShapeDtypeStruct((tokens, 2), jnp.int32),
        ),
        in_specs=[vmem] * 6,
        out_specs=(vmem, vmem, vmem),
        scratch_shapes=[pltpu.VMEM((tokens, width), BF16)],
        compiler_params=pltpu.CompilerParams(vmem_limit_bytes=48 * 2**20),
        name="prep",
    )(
        tokens_b,
        moe_gain.reshape(1, width),
        route_expert.T,
        route_expert,
        router_group,
        router_expert,
    )
    dma = pltpu.SemaphoreType.DMA
    pairs = nz // 2
    rows2 = 2 * nyc * sixteen
    slot = (nz, nyc, 2, sixteen, fq)
    mixer_out, moe_out = pl.pallas_call(
        functools.partial(moe_kernel, nz, nyc),
        out_shape=(
            jax.ShapeDtypeStruct((attended.shape[0], out_weight.shape[1]), BF16),
            jax.ShapeDtypeStruct((tokens // NTP, width), BF16),
        ),
        in_specs=[anywhere] * 6 + [vmem] * 2,
        out_specs=(vmem, vmem),
        scratch_shapes=[
            pltpu.VMEM(slot, BF16),
            pltpu.VMEM((NTP, *slot), BF16),
            pltpu.VMEM(expert_gate.shape, BF16),
            pltpu.VMEM(expert_up.shape, BF16),
            pltpu.VMEM((NTP, 2, hq, fq), BF16),
            pltpu.VMEM((NTP, pairs, 2, rows2, hq), BF16),
            pltpu.VMEM(slot, BF16),
            pltpu.VMEM(slot, BF16),
            pltpu.VMEM(slot, BF16),
            pltpu.VMEM((NTP, *attended.shape), BF16),
            pltpu.VMEM(out_weight.shape, BF16),
            pltpu.VMEM((NTP, tokens // NTP, fq), BF16),
            pltpu.VMEM((NTP, tokens // NTP, fq), BF16),
            dma((nz, 2)), dma((nz, 2)), dma((nz,)), dma((nz,)),
            dma((nz, 2)), dma((nz, 2)), dma((nz, 2)), dma((nz, 2)),
            dma((pairs, 2)), dma((pairs, 2)), dma((pairs, 2)), dma((pairs, 2)),
            dma((NTP,)), dma((NTP,)),
            dma((nz, 2)), dma((nz, 2)), dma((nz,)), dma((nz,)),
            dma((2,)), dma((2,)), dma((2,)), dma((2,)),
            dma((NTP,)), dma((NTP,)), dma((6,)),
        ],
        compiler_params=pltpu.CompilerParams(
            collective_id=0, has_side_effects=True, vmem_limit_bytes=60 * 2**20
        ),
        name="experts",
    )(slots, expert_gate, expert_up, expert_down, attended, out_weight, gates, rows)
    return (mixer_out, moe_out)


def solution(mesh):
    in_specs = (
        P("ep", "tp"),
        P("ep", "tp"),
        P("ep", "tp"),
        P("tp"),
        P(None, "tp"),
        P("ep", None),
        P(),
        P(),
        P(),
        P("ep", None),
        P("ep", None, "tp"),
        P("ep", None, "tp"),
        P("ep", "tp", None),
    )
    out_specs = (P("ep", "tp"), P(("ep", "tp"), None))
    return jax.shard_map(
        per_device, mesh=mesh, in_specs=in_specs, out_specs=out_specs, check_vma=False
    )
```

```python
import functools

import jax
import jax.numpy as jnp
from jax import lax
from jax.experimental import pallas as pl
from jax.experimental.pallas import tpu as pltpu
from jax.sharding import PartitionSpec as P

HEADS = 16
KV = 4
HD = 64
WINDOW = 128
CAP = 4
NTP = 4
PLANE = 8
MESH = pl.DeviceIdType.MESH
F32 = jnp.float32
BF16 = jnp.bfloat16


def hop_of(i, nz):
    if i == 0:
        return 0
    return (nz - i) // 2 if i % 2 == 0 else (i + nz - 1) // 2


def near_positions(nz):
    return [i for i in range(nz) if hop_of(i, nz) in (0, 1, nz - 1)]


def position_of(d, nz):
    return jnp.where(d == 0, 0, jnp.where(d < nz // 2, nz - 2 * d, 2 * d - nz + 1))


def slot_rows(expert, block, place, z, yc, nz, nyc):
    rank = expert >> 1
    d = ((rank >> (nyc.bit_length() - 1)) - z + nz) & (nz - 1)
    j = ((rank & (nyc - 1)) - yc + nyc) & (nyc - 1)
    return ((position_of(d, nz) * nyc + j) * 2 + (expert & 1)) * (NTP * CAP) + block * CAP + place


def iota(shape, dim):
    return lax.broadcasted_iota(jnp.int32, shape, dim)


def one_hot(hit):
    return jnp.where(hit, 1.0, 0.0).astype(BF16)


def dot_nt(a, b):
    return lax.dot_general(a, b, (((1,), (1,)), ((), ())), preferred_element_type=F32)


def step_kernel(
    nz, nyc, q_hbm, kt_hbm, vt_hbm, sink, ow_hbm, tok_hbm, gain, rgt, rex, rt, wg_hbm, wu_hbm, wd_hbm,
    mix, moe,
    tok, normed, slots, extra, relay, relay_e, arr, wg, wu, wq, act, out, back, ret, att, ow,
    fin_out, fin, gates, rows_in, qs, kvt, wide,
    zs, zr, zes, zer, ys, yr, yes, yer, xs, xr, fs, fr, acs, acr, afs, afr, ws, wr,
    rzs, rzr, rys, ryr, ts, tr, tfs, tfr, es, er, hs, hr, loc,
):
    x = lax.axis_index("tp")
    e = lax.axis_index("ep")
    z, yc = lax.div(e, nyc), lax.rem(e, nyc)
    fq = arr.shape[-1]
    hq = wg.shape[-1]
    hops = [hop_of(i, nz) for i in range(nz)]
    near = near_positions(nz)
    half = nyc // 2
    pairs = nz // 2
    tokens, width = tok.shape
    block_rows = tokens // NTP
    rest = pl.ds(1, nyc - 1)

    def zdev(d):
        return (lax.rem(z + (d + nz), nz) * nyc + yc, x)

    def ydev(j):
        return (z * nyc + lax.rem(yc + (j + nyc), nyc), x)

    def xdev(q):
        return (e, lax.rem(x + q, NTP))

    def edev(step):
        return (lax.rem(e + (step + nz * nyc), nz * nyc), x)

    def column(q):
        return lax.rem(x + (q + NTP), NTP)

    def send(src, dst, s_sem, r_sem, dev):
        copy = pltpu.make_async_remote_copy(
            src_ref=src, dst_ref=dst, send_sem=s_sem, recv_sem=r_sem,
            device_id=dev, device_id_type=MESH,
        )
        copy.start()

    def drain(ref, sem):
        pltpu.make_async_copy(ref, ref, sem).wait()

    def quarter(q, size):
        return pl.ds(pl.multiple_of(column(q) * size, size), size)

    barrier = pltpu.get_barrier_semaphore()
    peers = [xdev(q) for q in range(1, NTP)] + [edev(1), edev(-1)]
    peers += [ydev(j) for j in range(1, nyc)] + [zdev(d) for d in range(1, nz)]
    for peer in peers:
        pl.semaphore_signal(barrier, inc=1, device_id=peer, device_id_type=MESH)
    span = kt_hbm.shape[1]
    step = tokens // 4
    local = [
        pltpu.make_async_copy(wg_hbm, wg, loc.at[0]),
        pltpu.make_async_copy(wu_hbm, wu, loc.at[1]),
        pltpu.make_async_copy(wd_hbm.at[:, :, quarter(0, fq)], wq.at[0], loc.at[2]),
        pltpu.make_async_copy(ow_hbm, ow, loc.at[3]),
        pltpu.make_async_copy(q_hbm, qs, loc.at[4]),
        pltpu.make_async_copy(kt_hbm, kvt.at[0, :, pl.ds(WINDOW, span)], loc.at[5]),
        pltpu.make_async_copy(vt_hbm, kvt.at[1, :, pl.ds(WINDOW, span)], loc.at[6]),
    ]
    token_parts = [
        pltpu.make_async_copy(tok_hbm.at[pl.ds(i * step, step)], tok.at[pl.ds(i * step, step)], loc.at[7 + i])
        for i in range(4)
    ]
    for copy in token_parts + local:
        copy.start()
    pl.semaphore_wait(barrier, len(peers))

    for q in (1, 3, 2):
        send(wd_hbm.at[:, :, quarter(q, fq)], wq.at[q], ws.at[q], wr.at[q], xdev(q))
    tail = pl.ds(span - WINDOW, WINDOW)
    for w, source in enumerate((kt_hbm, vt_hbm)):
        send(source.at[:, tail], kvt.at[w, :, pl.ds(0, WINDOW)], hs.at[w], hr.at[w], edev(1))

    for i in range(4):
        token_parts[i].wait()

        def norm_rows(c, carry, i=i):
            where = pl.ds(pl.multiple_of(i * step + c * (step // 2), step // 2), step // 2)
            v = tok[where, :].astype(F32)
            ms = jnp.mean(v * v, axis=-1, keepdims=True)
            normed[where, :] = (v * lax.rsqrt(ms + 1e-06) * gain[...]).astype(BF16)
            return carry

        lax.fori_loop(0, 2, norm_rows, 0)

    experts = rex.shape[1]
    shift = block_rows.bit_length() - 1
    e0, e1 = rt[0:1, :], rt[1:2, :]
    ids = iota((experts, tokens), 0)
    hit0, hit1 = ids == e0, ids == e1
    first, second = iota((tokens, tokens), 0), iota((tokens, tokens), 1)
    before = one_hot(((first >> shift) == (second >> shift)) & (first < second))
    count = jnp.dot(one_hot(hit0 | hit1), before, preferred_element_type=F32)
    place0 = jnp.sum(jnp.where(hit0, count, 0.0), axis=0, keepdims=True).astype(jnp.int32)
    place1 = jnp.sum(jnp.where(hit1, count, 0.0), axis=0, keepdims=True).astype(jnp.int32)
    block = iota((1, tokens), 1) >> shift
    t0 = slot_rows(e0, block, place0, z, yc, nz, nyc)
    t1 = slot_rows(e1, block, place1, z, yc, nz, nyc)
    part = nyc * 2 * NTP * CAP

    def picked(i):
        ids = iota((part, tokens), 0) + i * part
        return one_hot((ids == t0) | (ids == t1))

    def filled(pick, q):
        got = jnp.dot(pick, normed[:, quarter(q, fq)], preferred_element_type=F32)
        return got.astype(BF16).reshape(nyc, 2, NTP * CAP, fq)

    def fill(i, carry):
        slots[i] = filled(picked(i), 0)
        return carry

    lax.fori_loop(0, nz, fill, 0)
    for i in range(1, nz):
        send(slots.at[i, rest], relay.at[i, rest], zs.at[i, 1], zr.at[i, 1], zdev(hops[i]))
        send(slots.at[i, 0], arr.at[0, i, 0], zs.at[i, 0], zr.at[i, 0], zdev(hops[i]))
    for j in range(1, nyc):
        send(slots.at[0, j], arr.at[0, 0, j], ys.at[0], yr.at[0], ydev(j))
    for f, i in enumerate(near):
        pick = picked(i)
        for q in range(1, NTP):
            extra[f, q - 1] = filled(pick, -q)
        for q in range(1, NTP):
            if i == 0:
                for j in range(1, nyc):
                    send(extra.at[f, q - 1, j], arr.at[q, 0, j], yes.at[f], yer.at[f], ydev(j))
                continue
            send(
                extra.at[f, q - 1, rest], relay_e.at[f, q - 1, rest],
                zes.at[f, q - 1, 1], zer.at[f, q - 1, 1], zdev(hops[i]),
            )
            send(
                extra.at[f, q - 1, 0], arr.at[q, i, 0],
                zes.at[f, q - 1, 0], zer.at[f, q - 1, 0], zdev(hops[i]),
            )
    arr[0, 0, 0] = slots[0, 0]
    for q in range(1, NTP):
        arr[q, 0, 0] = extra[0, q - 1, 0]

    lanes = iota((8, tokens), 0)
    table = jnp.zeros((8, tokens), F32)
    for at, value in enumerate((e0, e1, t0 >> 6, t0 & 63, t1 >> 6, t1 & 63)):
        table = jnp.where(lanes == at, value.astype(F32), table)
    turned = dot_nt(one_hot(first == second), table.astype(BF16)).astype(jnp.int32)
    c0, c1 = turned[:, 0:1], turned[:, 1:2]
    rows_in[:, 0:1] = turned[:, 2:3] * 64 + turned[:, 3:4]
    rows_in[:, 1:2] = turned[:, 4:5] * 64 + turned[:, 5:6]
    by_expert = jnp.dot(normed[...], rex[...], preferred_element_type=F32)
    by_group = dot_nt(normed[...], rgt[...])
    groups = rgt.shape[0]
    group_exp = jnp.exp(by_group - jnp.max(by_group, axis=1, keepdims=True))
    chosen = iota((tokens, groups), 1) == (c0 >> ((experts // groups).bit_length() - 1))
    share = jnp.sum(jnp.where(chosen, group_exp, 0.0), axis=1, keepdims=True) / jnp.sum(
        group_exp, axis=1, keepdims=True
    )
    ids = iota((tokens, experts), 1)
    l0 = jnp.sum(jnp.where(ids == c0, by_expert, 0.0), axis=1, keepdims=True)
    l1 = jnp.sum(jnp.where(ids == c1, by_expert, 0.0), axis=1, keepdims=True)
    top = jnp.maximum(l0, l1)
    x0, x1 = jnp.exp(l0 - top), jnp.exp(l1 - top)
    gates[:, 0:1] = share * (x0 / (x0 + x1))
    gates[:, 1:2] = share * (x1 / (x0 + x1))

    heads = qs.shape[1] // HD
    for copy in local[4:7]:
        copy.wait()
    for w in range(2):
        drain(kvt.at[w, :, pl.ds(0, WINDOW)], hr.at[w])
    for w in range(2):
        for h in range(heads):
            for other in range(heads):
                if other != h:
                    wide[w, h, pl.ds(other * HD, HD), :] = jnp.zeros((HD, span + WINDOW), BF16)
            wide[w, h, pl.ds(h * HD, HD), :] = kvt[w]

    def attend(b, carry):
        where = pl.ds(pl.multiple_of(b * WINDOW, WINDOW), WINDOW)
        band = pl.ds(pl.multiple_of(b * WINDOW, WINDOW), 2 * WINDOW)
        key = iota((WINDOW, 2 * WINDOW), 1)
        distance = iota((WINDOW, 2 * WINDOW), 0) + WINDOW - key
        earliest = jnp.where(e + b == 0, WINDOW, 0)
        allowed = (distance >= 0) & (distance < WINDOW) & (key >= earliest)
        queries = qs[where, :]
        total = jnp.zeros((WINDOW, heads * HD), F32)
        for h in range(heads):
            scores = jnp.dot(queries, wide[0, h, :, band], preferred_element_type=F32)
            masked = jnp.where(allowed, scores * HD ** (-0.5), -1e30)
            row_max = jnp.maximum(jnp.max(masked, axis=1, keepdims=True), sink[h])
            weights = jnp.exp(masked - row_max)
            denominator = jnp.sum(weights, axis=1, keepdims=True) + jnp.exp(sink[h] - row_max)
            probs = (weights / denominator).astype(BF16)
            total += dot_nt(probs, wide[1, h, :, band])
        att[0, where, :] = total.astype(BF16)
        return carry

    lax.fori_loop(0, span // WINDOW, attend, 0)

    def plane_out(i):
        if i == 0:
            return
        drain(relay.at[i, rest], zr.at[i, 1])
        for j in range(1, nyc):
            send(relay.at[i, j], arr.at[0, i, j], ys.at[i], yr.at[i], ydev(j))
        if i in near:
            f = near.index(i)
            for q in range(1, NTP):
                drain(relay_e.at[f, q - 1, rest], zer.at[f, q - 1, 1])
                for j in range(1, nyc):
                    send(relay_e.at[f, q - 1, j], arr.at[q, i, j], yes.at[f], yer.at[f], ydev(j))

    def ring_own(i):
        if i > 0:
            drain(arr.at[0, i, 0], zr.at[i, 0])
        drain(arr.at[0, i, rest], yr.at[i])
        if i in near:
            return
        send(arr.at[0, i], arr.at[1, i], xs.at[i, 0], xr.at[i, 0], xdev(1))
        send(arr.at[0, i], arr.at[3, i], xs.at[i, 1], xr.at[i, 1], xdev(3))

    low, high = pl.ds(0, half), pl.ds(half, half)

    def ring_on(i):
        if i in near:
            return
        drain(arr.at[1, i], xr.at[i, 0])
        send(arr.at[1, i, low], arr.at[2, i, low], fs.at[i, 0], fr.at[i, 0], xdev(1))
        drain(arr.at[3, i], xr.at[i, 1])
        send(arr.at[3, i, high], arr.at[2, i, high], fs.at[i, 1], fr.at[i, 1], xdev(3))

    def ring_in(i):
        if i in near:
            f = near.index(i)
            if i > 0:
                for q in range(1, NTP):
                    drain(arr.at[q, i, 0], zer.at[f, q - 1, 0])
            drain(arr.at[pl.ds(1, NTP - 1), i, rest], yer.at[f])
            return
        drain(arr.at[2, i, low], fr.at[i, 0])
        drain(arr.at[2, i, high], fr.at[i, 1])

    rows2 = 2 * nyc * NTP * CAP

    def hidden(p):
        if p == 0:
            local[0].wait()
            local[1].wait()

        def one(k, carry):
            gate = jnp.zeros((rows2, hq), F32)
            up = jnp.zeros((rows2, hq), F32)
            for q in range(NTP):
                depth = quarter(-q, fq)
                rows = arr[q, pl.ds(2 * p, 2), :, k].reshape(rows2, fq)
                gate += jnp.dot(rows, wg[k, depth, :], preferred_element_type=F32)
                up += jnp.dot(rows, wu[k, depth, :], preferred_element_type=F32)
            act[0, p, k] = (gate / (1.0 + jnp.exp(-gate)) * up).astype(BF16)
            return carry

        lax.fori_loop(0, 2, one, 0)
        send(act.at[0, p], act.at[1, p], acs.at[p, 0], acr.at[p, 0], xdev(1))
        send(act.at[0, p], act.at[3, p], acs.at[p, 1], acr.at[p, 1], xdev(3))

    def act_on(p):
        drain(act.at[1, p], acr.at[p, 0])
        send(act.at[1, p, 0], act.at[2, p, 0], afs.at[p, 0], afr.at[p, 0], xdev(1))
        drain(act.at[3, p], acr.at[p, 1])
        send(act.at[3, p, 1], act.at[2, p, 1], afs.at[p, 1], afr.at[p, 1], xdev(3))

    def down(p):
        if p == 0:
            local[2].wait()
            for q in range(1, NTP):
                drain(wq.at[q], wr.at[q])
        drain(act.at[2, p, 0], afr.at[p, 0])
        drain(act.at[2, p, 1], afr.at[p, 1])

        def one(k, carry):
            total = jnp.zeros((rows2, fq), F32)
            for q in range(NTP):
                total += jnp.dot(act[q, p, k], wq[q, k], preferred_element_type=F32)
            out[pl.ds(2 * p, 2), :, k] = total.astype(BF16).reshape(2, nyc, NTP * CAP, fq)
            return carry

        lax.fori_loop(0, 2, one, 0)
        for i in (2 * p, 2 * p + 1):
            if i == 0:
                ret[0, 0] = out[0, 0]
                for j in range(1, nyc):
                    send(out.at[0, j], ret.at[0, j], rys.at[0], ryr.at[0], ydev(-j))
                continue
            send(out.at[i, rest], back.at[i, rest], rzs.at[i, 1], rzr.at[i, 1], zdev(-hops[i]))
            send(out.at[i, 0], ret.at[i, 0], rzs.at[i, 0], rzr.at[i, 0], zdev(-hops[i]))

    def plane_back(i):
        if i == 0:
            return
        drain(back.at[i, rest], rzr.at[i, 1])
        for j in range(1, nyc):
            send(back.at[i, j], ret.at[i, j], rys.at[i], ryr.at[i], ydev(-j))

    for n in range(nz + 2):
        if n < nz:
            plane_out(n)
        if 0 <= n - 1 < nz:
            ring_own(n - 1)
        if 0 <= n - 2 < nz:
            ring_on(n - 2)
        m = n - 3
        if m >= 0:
            ring_in(m)
            if m % 2 == 1:
                hidden(m // 2)
                if m >= 3:
                    down(m // 2 - 1)
            elif m >= 2:
                act_on(m // 2 - 1)
    ring_in(nz - 1)
    hidden(pairs - 1)
    if pairs > 1:
        down(pairs - 2)
    act_on(pairs - 1)
    rows = att.shape[1]
    top, bottom = pl.ds(0, rows // 2), pl.ds(rows // 2, rows // 2)
    send(att.at[0], att.at[1], ts.at[0], tr.at[0], xdev(1))
    send(att.at[0], att.at[3], ts.at[1], tr.at[1], xdev(3))
    for i in range(nz - 4):
        plane_back(i)
    down(pairs - 1)
    for i in range(max(nz - 4, 0), nz - 2):
        plane_back(i)
    drain(att.at[1], tr.at[0])
    send(att.at[1, top], att.at[2, top], tfs.at[0], tfr.at[0], xdev(1))
    drain(att.at[3], tr.at[1])
    send(att.at[3, bottom], att.at[2, bottom], tfs.at[1], tfr.at[1], xdev(3))
    for i in range(nz - 2, nz):
        plane_back(i)
    local[3].wait()
    drain(att.at[2, top], tfr.at[0])
    drain(att.at[2, bottom], tfr.at[1])
    chunk = rows // 4
    hw = att.shape[2]

    def project(c, carry):
        where = pl.ds(pl.multiple_of(c * chunk, chunk), chunk)
        total = jnp.zeros((chunk, ow.shape[1]), F32)
        for q in range(NTP):
            total += jnp.dot(att[q, where, :], ow[quarter(-q, hw), :], preferred_element_type=F32)
        mix[where, :] = total.astype(BF16)
        return carry

    lax.fori_loop(0, 4, project, 0)

    for i in range(nz):
        if i > 0:
            drain(ret.at[i, 0], rzr.at[i, 0])
        drain(ret.at[i, rest], ryr.at[i])

    total_slots = nz * nyc * 2 * NTP * CAP

    def combined(t):
        where = pl.ds(pl.multiple_of(t * block_rows, block_rows), block_rows)
        ids = iota((block_rows, total_slots), 1)
        at = rows_in[where, :]
        pick = jnp.concatenate([one_hot(ids == at[:, k : k + 1]) for k in range(2)], axis=0)
        got = jnp.dot(pick, ret[...].reshape(total_slots, fq), preferred_element_type=F32)
        g = gates[where, :]
        return (g[:, 0:1] * got[:block_rows] + g[:, 1:2] * got[block_rows:]).astype(BF16)

    for q in (2, 1, 3):
        fin_out[q] = combined(column(q))
        send(fin_out.at[q], fin.at[q], es.at[q], er.at[q], xdev(q))
    moe[:, quarter(0, fq)] = combined(x)
    for q in range(1, NTP):
        drain(fin.at[q], er.at[q])
        moe[:, quarter(-q, fq)] = fin[q]

    for i in range(nz):
        if i > 0:
            drain(relay.at[i, 0], zs.at[i, 0])
            drain(relay.at[i, rest], zs.at[i, 1])
            drain(out.at[i, 0], rzs.at[i, 0])
            drain(out.at[i, rest], rzs.at[i, 1])
        drain(arr.at[0, i, rest], ys.at[i])
        drain(ret.at[i, rest], rys.at[i])
        if i in near:
            f = near.index(i)
            drain(arr.at[pl.ds(1, NTP - 1), i, rest], yes.at[f])
            if i > 0:
                for q in range(NTP - 1):
                    drain(relay.at[i, 0], zes.at[f, q, 0])
                    drain(relay.at[i, rest], zes.at[f, q, 1])
            continue
        for way in range(2):
            drain(arr.at[0, i], xs.at[i, way])
            drain(arr.at[0, i, low], fs.at[i, way])
    for p in range(pairs):
        for way in range(2):
            drain(act.at[0, p], acs.at[p, way])
            drain(act.at[0, p, 0], afs.at[p, way])
    for way in range(2):
        drain(att.at[0], ts.at[way])
        drain(att.at[0, top], tfs.at[way])
        drain(kvt.at[way, :, pl.ds(0, WINDOW)], hs.at[way])
    for q in range(1, NTP):
        drain(wq.at[q], ws.at[q])
        drain(fin_out.at[q], es.at[q])


def per_device(
    q_heads,
    k_heads,
    v_heads,
    sink_logits,
    out_weight,
    tokens_b,
    moe_gain,
    router_group,
    router_expert,
    route_expert,
    expert_gate,
    expert_up,
    expert_down,
):
    nyc = min(PLANE, lax.axis_size("ep"))
    nz = lax.axis_size("ep") // nyc
    tokens, width = tokens_b.shape
    fq = width // NTP
    hq = expert_gate.shape[2]
    sixteen = NTP * CAP
    span = q_heads.shape[0]
    vmem = pl.BlockSpec(memory_space=pltpu.VMEM)
    smem = pl.BlockSpec(memory_space=pltpu.SMEM)
    anywhere = pl.BlockSpec(memory_space=pl.ANY)
    dma = pltpu.SemaphoreType.DMA
    pairs = nz // 2
    near = len(near_positions(nz))
    rows2 = 2 * nyc * sixteen
    slot = (nz, nyc, 2, sixteen, fq)
    more = (near, NTP - 1, nyc, 2, sixteen, fq)
    return pl.pallas_call(
        functools.partial(step_kernel, nz, nyc),
        out_shape=(
            jax.ShapeDtypeStruct((span, out_weight.shape[1]), BF16),
            jax.ShapeDtypeStruct((tokens // NTP, width), BF16),
        ),
        in_specs=[anywhere] * 3 + [smem] + [anywhere] * 2 + [vmem] * 4 + [anywhere] * 3,
        out_specs=(vmem, vmem),
        scratch_shapes=[
            pltpu.VMEM(tokens_b.shape, BF16),
            pltpu.VMEM(tokens_b.shape, BF16),
            pltpu.VMEM(slot, BF16),
            pltpu.VMEM(more, BF16),
            pltpu.VMEM(slot, BF16),
            pltpu.VMEM(more, BF16),
            pltpu.VMEM((NTP, *slot), BF16),
            pltpu.VMEM(expert_gate.shape, BF16),
            pltpu.VMEM(expert_up.shape, BF16),
            pltpu.VMEM((NTP, 2, hq, fq), BF16),
            pltpu.VMEM((NTP, pairs, 2, rows2, hq), BF16),
            pltpu.VMEM(slot, BF16),
            pltpu.VMEM(slot, BF16),
            pltpu.VMEM(slot, BF16),
            pltpu.VMEM((NTP, *q_heads.shape), BF16),
            pltpu.VMEM(out_weight.shape, BF16),
            pltpu.VMEM((NTP, tokens // NTP, fq), BF16),
            pltpu.VMEM((NTP, tokens // NTP, fq), BF16),
            pltpu.VMEM((tokens, 2), F32),
            pltpu.VMEM((tokens, 2), jnp.int32),
            pltpu.VMEM(q_heads.shape, BF16),
            pltpu.VMEM((2, HD, span + WINDOW), BF16),
            pltpu.VMEM((2, q_heads.shape[1] // HD, q_heads.shape[1], span + WINDOW), BF16),
            dma((nz, 2)), dma((nz, 2)), dma((near, NTP - 1, 2)), dma((near, NTP - 1, 2)),
            dma((nz,)), dma((nz,)), dma((near,)), dma((near,)),
            dma((nz, 2)), dma((nz, 2)), dma((nz, 2)), dma((nz, 2)),
            dma((pairs, 2)), dma((pairs, 2)), dma((pairs, 2)), dma((pairs, 2)),
            dma((NTP,)), dma((NTP,)),
            dma((nz, 2)), dma((nz, 2)), dma((nz,)), dma((nz,)),
            dma((2,)), dma((2,)), dma((2,)), dma((2,)),
            dma((NTP,)), dma((NTP,)), dma((2,)), dma((2,)), dma((11,)),
        ],
        compiler_params=pltpu.CompilerParams(
            collective_id=0, has_side_effects=True, vmem_limit_bytes=62 * 2**20
        ),
        name="step",
    )(
        q_heads,
        k_heads.T,
        v_heads.T,
        sink_logits,
        out_weight,
        tokens_b,
        moe_gain.reshape(1, width),
        router_group.T,
        router_expert,
        route_expert.T,
        expert_gate,
        expert_up,
        expert_down,
    )


def solution(mesh):
    in_specs = (
        P("ep", "tp"),
        P("ep", "tp"),
        P("ep", "tp"),
        P("tp"),
        P(None, "tp"),
        P("ep", None),
        P(),
        P(),
        P(),
        P("ep", None),
        P("ep", None, "tp"),
        P("ep", None, "tp"),
        P("ep", "tp", None),
    )
    out_specs = (P("ep", "tp"), P(("ep", "tp"), None))
    return jax.shard_map(
        per_device, mesh=mesh, in_specs=in_specs, out_specs=out_specs, check_vma=False
    )
```

```python
import functools

import jax
import jax.numpy as jnp
from jax import lax
from jax.experimental import pallas as pl
from jax.experimental.pallas import tpu as pltpu
from jax.sharding import PartitionSpec as P

HEADS = 16
KV = 4
HD = 64
WINDOW = 128
CAP = 4
NTP = 4
PLANE = 8
GROUPS = 4
NEAR = (0, 1, 7)
TWO = (2, 6)
MESSAGES = [(1, 0), (2, 0), (3, 0), (4, 0), (5, 0), (4, 2), (5, 2), (6, 0), (7, 0)]
CHUNKS = [(1, 2), (3, 1), (4, 2), (6, 2), (0, 1)]
MIDDLE = (
    "Z0", "Z1", "O1", "Z2", "O2", "Z-1", "O3", "Z3", "F1", "Z4", "Z5", "Z6", "F2", "F3", "O4", "Z7",
    "I1", "I2", "H0", "Z8", "I3", "H1", "O5", "A0", "A1", "I4", "I5", "H2", "D0", "D1", "I6", "I7",
    "H3", "A2", "I0", "H4", "B1", "B2", "B3", "A3", "D2", "A4", "T0", "D3", "B4", "B5",
)
TAIL = (
    "D4", "B6", "B7", "B0", "T1",
)
AHEAD = 2
MESH = pl.DeviceIdType.MESH
F32 = jnp.float32
BF16 = jnp.bfloat16


def hop_of(i, nz):
    return ([0, 3, 5, 4, 2, 6, 1, 7])[i] if nz == 8 else i


def near_positions(nz):
    return [i for i in range(nz) if hop_of(i, nz) in NEAR]


def plain_chunks(nz):
    return [(2 * p, 2) for p in range(nz // 2)]


def slot_entries(nz):
    near = near_positions(nz)
    kinds = [range(NTP) if i in near else (0, 2) if hop_of(i, nz) in TWO else (0,) for i in range(nz)]
    return [(i, q) for i in range(nz) for q in kinds[i]]


def plain_messages(far, two, near):
    return [(i, 0) for i in far] + [(i, 2) for i in two] + [(i, 0) for i in near if i > 0]


def plain_order(messages, far, two, nz):
    steps = [f"Z{k}" for k in range(len(messages))] + [f"O{i}" for i in far]
    steps += [f"F{i}" for i in far if i not in two]
    steps += [f"I{i}" for i in range(nz)]
    for p in range(nz // 2):
        steps += [f"H{p}", f"A{p}"]
        if p < nz // 2 - 1:
            steps += [f"D{p}", f"B{2 * p}", f"B{2 * p + 1}"]
    return steps


def iota(shape, dim):
    return lax.broadcasted_iota(jnp.int32, shape, dim)


def one_hot(hit):
    return jnp.where(hit, 1.0, 0.0).astype(BF16)


def dot_nt(a, b):
    return lax.dot_general(a, b, (((1,), (1,)), ((), ())), preferred_element_type=F32)


def step_kernel(
    nz, nyc, q_hbm, kt_hbm, vt_hbm, sink, ow_hbm, tok_hbm, gain_hbm, rgt_hbm, rex_hbm, rt_hbm,
    wg_hbm, wu_hbm, wd_hbm, mix_hbm, moe,
    gain, rgt, rex, rt, mix,
    tok, normed, comp, meta, order, cin, cin_e, min_, mcol, relay, arr, wg, wu, wq, act,
    out, back, pout, rtok, att, ow, fin_out, fin, qs, kvt, wide,
    zs, zr, ms, mr, ys, yr, yes, yer, xs, xr, fs, fr, acs, acr, afs, afr, ws, wr,
    rzs, rzr, rys, ryr, ts, tr, tfs, tfr, es, er, hs, hr, loc,
):
    x = lax.axis_index("tp")
    e = lax.axis_index("ep")
    z, yc = lax.div(e, nyc), lax.rem(e, nyc)
    fq = arr.shape[-1]
    hq = wg.shape[-1]
    hops = [hop_of(i, nz) for i in range(nz)]
    near = near_positions(nz)
    half = nyc // 2
    chunks = CHUNKS if nz == 8 else plain_chunks(nz)
    tokens, width = tok.shape
    block_rows = tokens // NTP
    rest = pl.ds(1, nyc - 1)

    def zdev(d):
        return (lax.rem(z + (d + nz), nz) * nyc + yc, x)

    def ydev(j):
        return (z * nyc + lax.rem(yc + (j + nyc), nyc), x)

    def xdev(q):
        return (e, lax.rem(x + q, NTP))

    def edev(step):
        return (lax.rem(e + (step + nz * nyc), nz * nyc), x)

    def column(q):
        return lax.rem(x + (q + NTP), NTP)

    def send(src, dst, s_sem, r_sem, dev):
        copy = pltpu.make_async_remote_copy(
            src_ref=src, dst_ref=dst, send_sem=s_sem, recv_sem=r_sem,
            device_id=dev, device_id_type=MESH,
        )
        copy.start()

    def drain(ref, sem):
        pltpu.make_async_copy(ref, ref, sem).wait()

    def quarter(q, size):
        return pl.ds(pl.multiple_of(column(q) * size, size), size)

    barrier = pltpu.get_barrier_semaphore()
    peers = [xdev(q) for q in range(1, NTP)] + [edev(1), edev(-1)]
    peers += [ydev(j) for j in range(1, nyc)] + [zdev(d) for d in range(1, nz)]
    for peer in peers:
        pl.semaphore_signal(barrier, inc=1, device_id=peer, device_id_type=MESH)
    span = kt_hbm.shape[1]
    step = tokens // 4
    local = [
        pltpu.make_async_copy(wg_hbm, wg, loc.at[0]),
        pltpu.make_async_copy(wu_hbm, wu, loc.at[1]),
        pltpu.make_async_copy(wd_hbm.at[:, :, quarter(0, fq)], wq.at[0], loc.at[2]),
        pltpu.make_async_copy(ow_hbm, ow, loc.at[3]),
        pltpu.make_async_copy(q_hbm, qs, loc.at[4]),
        pltpu.make_async_copy(kt_hbm, kvt.at[0, :, pl.ds(WINDOW, span)], loc.at[5]),
        pltpu.make_async_copy(vt_hbm, kvt.at[1, :, pl.ds(WINDOW, span)], loc.at[6]),
    ]
    token_parts = [
        pltpu.make_async_copy(tok_hbm.at[pl.ds(i * step, step)], tok.at[pl.ds(i * step, step)], loc.at[7 + i])
        for i in range(4)
    ]
    small = [
        pltpu.make_async_copy(source, target, loc.at[11 + n])
        for n, (source, target) in enumerate(
            ((gain_hbm, gain), (rt_hbm, rt), (rgt_hbm, rgt), (rex_hbm, rex))
        )
    ]
    for copy in token_parts + small + local:
        copy.start()
    pl.semaphore_wait(barrier, len(peers))

    for q in (1, 3, 2):
        send(wd_hbm.at[:, :, quarter(q, fq)], wq.at[q], ws.at[q], wr.at[q], xdev(q))
    tail = pl.ds(span - WINDOW, WINDOW)
    for w, source in enumerate((kt_hbm, vt_hbm)):
        send(source.at[:, tail], kvt.at[w, :, pl.ds(0, WINDOW)], hs.at[w], hr.at[w], edev(1))

    for copy in small:
        copy.wait()
    for i in range(4):
        token_parts[i].wait()

        def norm_rows(c, carry, i=i):
            where = pl.ds(pl.multiple_of(i * step + c * (step // 2), step // 2), step // 2)
            v = tok[where, :].astype(F32)
            ms = jnp.mean(v * v, axis=-1, keepdims=True)
            normed[where, :] = (v * lax.rsqrt(ms + 1e-06) * gain[...]).astype(BF16)
            return carry

        lax.fori_loop(0, 2, norm_rows, 0)

    experts = rex.shape[1]
    shift = block_rows.bit_length() - 1
    per_group = block_rows // GROUPS
    group_rows = tokens // GROUPS
    planes = nz // GROUPS
    part = nyc * 2 * NTP * CAP
    e0, e1 = rt[0:1, :], rt[1:2, :]
    ids = iota((experts, tokens), 0)
    hit0, hit1 = ids == e0, ids == e1
    first, second = iota((tokens, tokens), 0), iota((tokens, tokens), 1)
    before = one_hot(((first >> shift) == (second >> shift)) & (first < second))
    count = jnp.dot(one_hot(hit0 | hit1), before, preferred_element_type=F32)
    place0 = jnp.sum(jnp.where(hit0, count, 0.0), axis=0, keepdims=True).astype(jnp.int32)
    place1 = jnp.sum(jnp.where(hit1, count, 0.0), axis=0, keepdims=True).astype(jnp.int32)
    group = e0 >> ((experts // GROUPS).bit_length() - 1)
    mine = iota((16, tokens), 0) == group
    count = jnp.dot(one_hot(mine), before, preferred_element_type=F32)
    nth = jnp.sum(jnp.where(mine, count, 0.0), axis=0, keepdims=True).astype(jnp.int32)
    block = iota((1, tokens), 1) >> shift
    in_block = group * per_group + nth
    place = group * group_rows + block * per_group + nth

    def compact(c, carry):
        where = pl.ds(pl.multiple_of(c * group_rows, group_rows), group_rows)
        pick = one_hot(iota((group_rows, tokens), 0) + c * group_rows == place)
        comp[where, :] = jnp.dot(pick, normed[...], preferred_element_type=F32).astype(BF16)
        return carry

    lax.fori_loop(0, GROUPS, compact, 0)

    def group_at(d):
        g = lax.div(lax.rem(z + (d + nz), nz), planes)
        return pl.ds(pl.multiple_of(g * group_rows, group_rows), group_rows)

    far = [i for i in range(nz) if i not in near]
    two = [i for i in far if hops[i] in TWO]
    messages = MESSAGES if nz == 8 else plain_messages(far, two, near)
    entries = slot_entries(nz)

    def plane_send(k):
        i, q = messages[k]
        if i in near:
            source, target = comp.at[group_at(hops[i]), :], cin_e.at[near.index(i)]
        else:
            source, target = comp.at[group_at(hops[i]), quarter(-q, fq)], cin.at[i, q // 2]
        send(source, target, zs.at[k], zr.at[k], zdev(hops[i]))

    for k in range(min(AHEAD, len(messages))):
        plane_send(k)

    by_expert = lax.dot_general(
        rex[...], normed[...], (((0,), (1,)), ((), ())), preferred_element_type=F32
    )
    by_group = dot_nt(rgt[...], normed[...])
    groups = rgt.shape[0]
    group_exp = jnp.exp(by_group - jnp.max(by_group, axis=0, keepdims=True))
    chosen = iota((groups, tokens), 0) == group
    share = jnp.sum(jnp.where(chosen, group_exp, 0.0), axis=0, keepdims=True) / jnp.sum(
        group_exp, axis=0, keepdims=True
    )
    l0 = jnp.sum(jnp.where(hit0, by_expert, 0.0), axis=0, keepdims=True)
    l1 = jnp.sum(jnp.where(hit1, by_expert, 0.0), axis=0, keepdims=True)
    top = jnp.maximum(l0, l1)
    x0, x1 = jnp.exp(l0 - top), jnp.exp(l1 - top)

    def plane_row(expert, place):
        j = (((expert >> 1) & (nyc - 1)) - yc + nyc) & (nyc - 1)
        return (j * 2 + (expert & 1)) * (NTP * CAP) + block * CAP + place

    def plane_of(expert):
        return expert >> nyc.bit_length()

    def pieces(value):
        high = value.astype(BF16).astype(F32)
        middle = (value - high).astype(BF16).astype(F32)
        return (high, middle, value - high - middle)

    values = [plane_row(e0, place0), plane_row(e1, place1), plane_of(e0), plane_of(e1)]
    values += [*pieces(share * (x0 / (x0 + x1))), *pieces(share * (x1 / (x0 + x1)))]
    lanes = iota((16, tokens), 0)
    table = jnp.zeros((16, tokens), F32)
    for at, value in enumerate(values):
        table = jnp.where(lanes == at, value.astype(F32), table)
    spread = one_hot(first == place)
    turned = dot_nt(table.astype(BF16), spread)
    for g in range(GROUPS):
        meta[g] = turned[:, g * group_rows : (g + 1) * group_rows]
    order[...] = jnp.broadcast_to(in_block.astype(F32), order.shape)
    for i in range(1, nz):
        g = lax.div(lax.rem(z + (hops[i] + nz), nz), planes)
        send(meta.at[g], min_.at[i], ms.at[i], mr.at[i], zdev(hops[i]))
    min_[0] = meta[lax.div(z, planes)]

    eye = one_hot(iota((group_rows, group_rows), 0) == iota((group_rows, group_rows), 1))

    def plane_out(k):
        i, first_q = (0, 0) if k < 0 else messages[k]
        if i > 0:
            drain(cin_e.at[near.index(i)] if i in near else cin.at[i, first_q // 2], zr.at[k])
            if k + AHEAD < len(messages):
                plane_send(k + AHEAD)
            if first_q == 0:
                drain(min_.at[i], mr.at[i])
        given = min_[i]
        if first_q == 0:
            mcol[i] = dot_nt(eye, given.astype(BF16))
        row0 = jnp.where(given[2:3, :].astype(jnp.int32) == z, given[0:1, :].astype(jnp.int32), -1)
        row1 = jnp.where(given[3:4, :].astype(jnp.int32) == z, given[1:2, :].astype(jnp.int32), -1)
        ids = iota((part, group_rows), 0)
        pick = one_hot((ids == row0) | (ids == row1))
        for q in range(NTP) if i in near else (first_q,):
            if i == 0:
                rows = comp[group_at(0), quarter(-q, fq)]
            elif i in near:
                rows = cin_e[near.index(i), :, quarter(-q, fq)]
            else:
                rows = cin[i, q // 2]
            got = jnp.dot(pick, rows, preferred_element_type=F32).astype(BF16)
            got = got.reshape(nyc, 2, NTP * CAP, fq)
            at = entries.index((i, q))
            arr[q, i, 0] = got[0]
            relay[at, rest] = got[1:]
            for j in range(1, nyc):
                if q == 0:
                    send(relay.at[at, j], arr.at[0, i, j], ys.at[i], yr.at[i], ydev(j))
                else:
                    send(relay.at[at, j], arr.at[q, i, j], yes.at[i], yer.at[i], ydev(j))

    def others(i):
        if i in near:
            return arr.at[pl.ds(1, NTP - 1), i, rest]
        return arr.at[2, i, rest]

    heads = qs.shape[1] // HD
    for copy in local[4:7]:
        copy.wait()
    for w in range(2):
        drain(kvt.at[w, :, pl.ds(0, WINDOW)], hr.at[w])
    for w in range(2):
        for h in range(heads):
            for other in range(heads):
                if other != h:
                    wide[w, h, pl.ds(other * HD, HD), :] = jnp.zeros((HD, span + WINDOW), BF16)
            wide[w, h, pl.ds(h * HD, HD), :] = kvt[w]

    def attend(b, carry):
        where = pl.ds(pl.multiple_of(b * WINDOW, WINDOW), WINDOW)
        band = pl.ds(pl.multiple_of(b * WINDOW, WINDOW), 2 * WINDOW)
        key = iota((WINDOW, 2 * WINDOW), 1)
        distance = iota((WINDOW, 2 * WINDOW), 0) + WINDOW - key
        earliest = jnp.where(e + b == 0, WINDOW, 0)
        allowed = (distance >= 0) & (distance < WINDOW) & (key >= earliest)
        queries = qs[where, :]
        total = jnp.zeros((WINDOW, heads * HD), F32)
        for h in range(heads):
            scores = jnp.dot(queries, wide[0, h, :, band], preferred_element_type=F32)
            masked = jnp.where(allowed, scores * HD ** (-0.5), -1e30)
            row_max = jnp.maximum(jnp.max(masked, axis=1, keepdims=True), sink[h])
            weights = jnp.exp(masked - row_max)
            denominator = jnp.sum(weights, axis=1, keepdims=True) + jnp.exp(sink[h] - row_max)
            probs = (weights / denominator).astype(BF16)
            total += dot_nt(probs, wide[1, h, :, band])
        att[0, where, :] = total.astype(BF16)
        return carry

    lax.fori_loop(0, span // WINDOW, attend, 0)

    def ring_own(i):
        drain(arr.at[0, i, rest], yr.at[i])
        send(arr.at[0, i], arr.at[1, i], xs.at[i, 0], xr.at[i, 0], xdev(1))
        send(arr.at[0, i], arr.at[3, i], xs.at[i, 1], xr.at[i, 1], xdev(3))

    low, high = pl.ds(0, half), pl.ds(half, half)

    def ring_on(i):
        drain(arr.at[1, i], xr.at[i, 0])
        send(arr.at[1, i, low], arr.at[2, i, low], fs.at[i, 0], fr.at[i, 0], xdev(1))
        drain(arr.at[3, i], xr.at[i, 1])
        send(arr.at[3, i, high], arr.at[2, i, high], fs.at[i, 1], fr.at[i, 1], xdev(3))

    def ring_in(i):
        if i in near:
            drain(arr.at[0, i, rest], yr.at[i])
        elif i in two:
            drain(arr.at[1, i], xr.at[i, 0])
            drain(arr.at[3, i], xr.at[i, 1])
        else:
            drain(arr.at[2, i, low], fr.at[i, 0])
            drain(arr.at[2, i, high], fr.at[i, 1])
            return
        drain(others(i), yer.at[i])

    rows1 = nyc * NTP * CAP

    def span_of(c):
        first, many = chunks[c]
        return pl.ds(first, many), many * rows1

    def hidden(c):
        if c == 0:
            local[0].wait()
            local[1].wait()
        span, rows2 = span_of(c)

        def one(k, carry):
            gate = jnp.zeros((rows2, hq), F32)
            up = jnp.zeros((rows2, hq), F32)
            for q in range(NTP):
                depth = quarter(-q, fq)
                rows = arr[q, span, :, k].reshape(rows2, fq)
                gate += jnp.dot(rows, wg[k, depth, :], preferred_element_type=F32)
                up += jnp.dot(rows, wu[k, depth, :], preferred_element_type=F32)
            value = (gate / (1.0 + jnp.exp(-gate)) * up).astype(BF16)
            act[0, span, k] = value.reshape(-1, rows1, hq)
            return carry

        lax.fori_loop(0, 2, one, 0)
        send(act.at[0, span], act.at[1, span], acs.at[c, 0], acr.at[c, 0], xdev(1))
        send(act.at[0, span], act.at[3, span], acs.at[c, 1], acr.at[c, 1], xdev(3))

    def act_on(c):
        span, _ = span_of(c)
        drain(act.at[1, span], acr.at[c, 0])
        send(act.at[1, span, 0], act.at[2, span, 0], afs.at[c, 0], afr.at[c, 0], xdev(1))
        drain(act.at[3, span], acr.at[c, 1])
        send(act.at[3, span, 1], act.at[2, span, 1], afs.at[c, 1], afr.at[c, 1], xdev(3))

    def down(c):
        if c == 0:
            local[2].wait()
            for q in range(1, NTP):
                drain(wq.at[q], wr.at[q])
        span, rows2 = span_of(c)
        drain(act.at[2, span, 0], afr.at[c, 0])
        drain(act.at[2, span, 1], afr.at[c, 1])

        def one(k, carry):
            total = jnp.zeros((rows2, fq), F32)
            for q in range(NTP):
                rows = act[q, span, k].reshape(rows2, hq)
                total += jnp.dot(rows, wq[q, k], preferred_element_type=F32)
            out[span, :, k] = total.astype(BF16).reshape(-1, nyc, NTP * CAP, fq)
            return carry

        lax.fori_loop(0, 2, one, 0)
        for i in range(chunks[c][0], sum(chunks[c])):
            for j in range(1, nyc):
                send(out.at[i, j], back.at[i, j], rys.at[i], ryr.at[i], ydev(-j))
            back[i, 0] = out[i, 0]

    def plane_back(i):
        drain(back.at[i, rest], ryr.at[i])
        given = mcol[i]
        ids = iota((group_rows, part), 1)
        picks = []
        for k in range(2):
            row = given[:, k : k + 1].astype(jnp.int32)
            here = given[:, 2 + k : 3 + k].astype(jnp.int32) == z
            picks.append(one_hot(ids == jnp.where(here, row, -1)))
        got = jnp.dot(
            jnp.concatenate(picks, axis=0), back[i].reshape(part, fq), preferred_element_type=F32
        )
        g0 = given[:, 4:5] + given[:, 5:6] + given[:, 6:7]
        g1 = given[:, 7:8] + given[:, 8:9] + given[:, 9:10]
        total = (g0 * got[:group_rows] + g1 * got[group_rows:]).astype(BF16)
        if i == 0:
            rtok[0] = total
            return
        pout[i] = total
        send(pout.at[i], rtok.at[hops[i]], rzs.at[i], rzr.at[i], zdev(-hops[i]))

    rows = att.shape[1]
    top_half, low_half = pl.ds(0, rows // 2), pl.ds(rows // 2, rows // 2)

    def heads_ring(part):
        if part == 0:
            send(att.at[0], att.at[1], ts.at[0], tr.at[0], xdev(1))
            send(att.at[0], att.at[3], ts.at[1], tr.at[1], xdev(3))
            return
        drain(att.at[1], tr.at[0])
        send(att.at[1, top_half], att.at[2, top_half], tfs.at[0], tfr.at[0], xdev(1))
        drain(att.at[3], tr.at[1])
        send(att.at[3, low_half], att.at[2, low_half], tfs.at[1], tfr.at[1], xdev(3))

    steps = {
        "Z": plane_out, "O": ring_own, "F": ring_on, "I": ring_in, "H": hidden,
        "A": act_on, "D": down, "B": plane_back, "T": heads_ring,
    }
    for step in MIDDLE if nz == 8 else plain_order(messages, far, two, nz):
        steps[step[0]](int(step[1:]))
    for step in TAIL if nz == 8 else ("T0", f"D{len(chunks) - 1}", f"B{nz - 2}", f"B{nz - 1}", "T1"):
        steps[step[0]](int(step[1:]))
    local[3].wait()
    chunk = rows // 4
    hw = att.shape[2]

    def project(c, carry):
        where = pl.ds(pl.multiple_of(c * chunk, chunk), chunk)
        total = jnp.zeros((chunk, ow.shape[1]), F32)
        for q in range(NTP):
            total += jnp.dot(att[q, where, :], ow[quarter(-q, hw), :], preferred_element_type=F32)
        mix[where, :] = total.astype(BF16)
        return carry

    for i in range(1, nz):
        drain(rtok.at[hops[i]], rzr.at[i])

    def combined(t):
        where = pl.ds(pl.multiple_of(t * per_group, per_group), per_group)
        found = []
        for g in range(GROUPS):
            total = jnp.zeros((per_group, fq), F32)
            for p in range(planes):
                d = lax.rem(g * planes + p + nz - z, nz)
                total += rtok[d, where, :].astype(F32)
            found.append(total.astype(BF16))
        return jnp.concatenate(found, axis=0)

    for q in (2, 1, 3):
        fin_out[q] = combined(column(q))
        send(fin_out.at[q], fin.at[q], es.at[q], er.at[q], xdev(q))
    drain(att.at[2, top_half], tfr.at[0])
    drain(att.at[2, low_half], tfr.at[1])
    lax.fori_loop(0, 4, project, 0)
    mixed = pltpu.make_async_copy(mix, mix_hbm, loc.at[15])
    mixed.start()
    own = combined(x)
    turned = order[:, pl.ds(pl.multiple_of(x * block_rows, block_rows), block_rows)]
    rows, cols = iota((block_rows, block_rows), 0), iota((block_rows, block_rows), 1)
    turned = dot_nt(one_hot(rows == cols), turned.astype(BF16)).astype(jnp.int32)
    spread = one_hot(cols == turned[:, 0:1])
    moe[:, quarter(0, fq)] = jnp.dot(spread, own, preferred_element_type=F32).astype(BF16)
    for q in (1, 3, 2):
        drain(fin.at[q], er.at[q])
        placed = jnp.dot(spread, fin[q], preferred_element_type=F32).astype(BF16)
        moe[:, quarter(-q, fq)] = placed

    mixed.wait()
    for k, (i, q) in enumerate(messages):
        drain(cin_e.at[near.index(i)] if i in near else cin.at[i, q // 2], zs.at[k])
    for i in range(nz):
        drain(arr.at[0, i, rest], ys.at[i])
        if i in near or i in two:
            drain(others(i), yes.at[i])
        drain(back.at[i, rest], rys.at[i])
        if i > 0:
            drain(min_.at[i], ms.at[i])
            drain(pout.at[i], rzs.at[i])
        if i in near:
            continue
        for way in range(2):
            drain(arr.at[0, i], xs.at[i, way])
            if i not in two:
                drain(arr.at[0, i, low], fs.at[i, way])
    for c in range(len(chunks)):
        span, _ = span_of(c)
        for way in range(2):
            drain(act.at[0, span], acs.at[c, way])
            drain(act.at[0, span, 0], afs.at[c, way])
    for way in range(2):
        drain(att.at[0], ts.at[way])
        drain(att.at[0, top_half], tfs.at[way])
        drain(kvt.at[way, :, pl.ds(0, WINDOW)], hs.at[way])
    for q in range(1, NTP):
        drain(wq.at[q], ws.at[q])
        drain(fin_out.at[q], es.at[q])


def per_device(
    q_heads,
    k_heads,
    v_heads,
    sink_logits,
    out_weight,
    tokens_b,
    moe_gain,
    router_group,
    router_expert,
    route_expert,
    expert_gate,
    expert_up,
    expert_down,
):
    nyc = min(PLANE, lax.axis_size("ep"))
    nz = lax.axis_size("ep") // nyc
    tokens, width = tokens_b.shape
    fq = width // NTP
    hq = expert_gate.shape[2]
    sixteen = NTP * CAP
    span = q_heads.shape[0]
    vmem = pl.BlockSpec(memory_space=pltpu.VMEM)
    smem = pl.BlockSpec(memory_space=pltpu.SMEM)
    anywhere = pl.BlockSpec(memory_space=pl.ANY)
    dma = pltpu.SemaphoreType.DMA
    chunks = len(CHUNKS if nz == 8 else plain_chunks(nz))
    near = len(near_positions(nz))
    slot = (nz, nyc, 2, sixteen, fq)
    group_rows = tokens // GROUPS
    return pl.pallas_call(
        functools.partial(step_kernel, nz, nyc),
        out_shape=(
            jax.ShapeDtypeStruct((span, out_weight.shape[1]), BF16),
            jax.ShapeDtypeStruct((tokens // NTP, width), BF16),
        ),
        in_specs=[anywhere] * 3 + [smem] + [anywhere] * 9,
        out_specs=(anywhere, vmem),
        scratch_shapes=[
            pltpu.VMEM((1, width), F32),
            pltpu.VMEM((router_group.shape[1], width), BF16),
            pltpu.VMEM(router_expert.shape, BF16),
            pltpu.VMEM((2, tokens), jnp.int32),
            pltpu.VMEM((span, out_weight.shape[1]), BF16),
            pltpu.VMEM(tokens_b.shape, BF16),
            pltpu.VMEM(tokens_b.shape, BF16),
            pltpu.VMEM(tokens_b.shape, BF16),
            pltpu.VMEM((GROUPS, 16, group_rows), F32),
            pltpu.VMEM((8, tokens), F32),
            pltpu.VMEM((nz, 2, group_rows, fq), BF16),
            pltpu.VMEM((near, group_rows, width), BF16),
            pltpu.VMEM((nz, 16, group_rows), F32),
            pltpu.VMEM((nz, group_rows, 16), F32),
            pltpu.VMEM((len(slot_entries(nz)), *slot[1:]), BF16),
            pltpu.VMEM((NTP, *slot), BF16),
            pltpu.VMEM(expert_gate.shape, BF16),
            pltpu.VMEM(expert_up.shape, BF16),
            pltpu.VMEM((NTP, 2, hq, fq), BF16),
            pltpu.VMEM((NTP, nz, 2, nyc * sixteen, hq), BF16),
            pltpu.VMEM(slot, BF16),
            pltpu.VMEM(slot, BF16),
            pltpu.VMEM((nz, group_rows, fq), BF16),
            pltpu.VMEM((nz, group_rows, fq), BF16),
            pltpu.VMEM((NTP, *q_heads.shape), BF16),
            pltpu.VMEM(out_weight.shape, BF16),
            pltpu.VMEM((NTP, tokens // NTP, fq), BF16),
            pltpu.VMEM((NTP, tokens // NTP, fq), BF16),
            pltpu.VMEM(q_heads.shape, BF16),
            pltpu.VMEM((2, HD, span + WINDOW), BF16),
            pltpu.VMEM((2, q_heads.shape[1] // HD, q_heads.shape[1], span + WINDOW), BF16),
            dma((2 * nz,)), dma((2 * nz,)), dma((nz,)), dma((nz,)),
            dma((nz,)), dma((nz,)), dma((nz,)), dma((nz,)),
            dma((nz, 2)), dma((nz, 2)), dma((nz, 2)), dma((nz, 2)),
            dma((chunks, 2)), dma((chunks, 2)), dma((chunks, 2)), dma((chunks, 2)),
            dma((NTP,)), dma((NTP,)),
            dma((nz,)), dma((nz,)), dma((nz,)), dma((nz,)),
            dma((2,)), dma((2,)), dma((2,)), dma((2,)),
            dma((NTP,)), dma((NTP,)), dma((2,)), dma((2,)), dma((16,)),
        ],
        compiler_params=pltpu.CompilerParams(
            collective_id=0, has_side_effects=True, vmem_limit_bytes=62 * 2**20
        ),
        name="step",
    )(
        q_heads,
        k_heads.T,
        v_heads.T,
        sink_logits,
        out_weight,
        tokens_b,
        moe_gain.reshape(1, width),
        router_group.T,
        router_expert,
        route_expert.T,
        expert_gate,
        expert_up,
        expert_down,
    )


def solution(mesh):
    in_specs = (
        P("ep", "tp"),
        P("ep", "tp"),
        P("ep", "tp"),
        P("tp"),
        P(None, "tp"),
        P("ep", None),
        P(),
        P(),
        P(),
        P("ep", None),
        P("ep", None, "tp"),
        P("ep", None, "tp"),
        P("ep", "tp", None),
    )
    out_specs = (P("ep", "tp"), P(("ep", "tp"), None))
    return jax.shard_map(
        per_device, mesh=mesh, in_specs=in_specs, out_specs=out_specs, check_vma=False
    )
```

```python
import functools

import jax
import jax.numpy as jnp
from jax import lax
from jax.experimental import pallas as pl
from jax.experimental.pallas import tpu as pltpu
from jax.sharding import PartitionSpec as P

HEADS = 16
KV = 4
HD = 64
WINDOW = 128
CAP = 4
NTP = 4
PLANE = 8
GROUPS = 4
NEAR = (0, 1, 7)
TWO = (2, 6)
MESSAGES = [(1, 0), (2, 0), (3, 0), (4, 0), (5, 0), (4, 2), (5, 2), (6, 0), (7, 0)]
CHUNKS = [(1, 2), (3, 1), (4, 2), (6, 2), (0, 1)]
MIDDLE = (
    "Z0", "Z1", "O1", "Z2", "O2", "Z-1", "O3", "Z3", "F1", "Z4", "Z5", "Z6", "F2", "F3", "O4", "Z7",
    "I1", "I2", "H0", "Z8", "I3", "H1", "O5", "A0", "A1", "I4", "I5", "H2", "D0", "D1", "I6", "I7",
    "H3", "A2", "I0", "H4", "B1", "B2", "B3", "A3", "D2", "A4", "T0", "D3", "B4", "B5",
)
TAIL = (
    "D4", "B6", "B7", "B0", "T1",
)
AHEAD = 2
WIDEN = 2
MESH = pl.DeviceIdType.MESH
F32 = jnp.float32
BF16 = jnp.bfloat16


def hop_of(i, nz):
    return ([0, 3, 5, 4, 2, 6, 1, 7])[i] if nz == 8 else i


def near_positions(nz):
    return [i for i in range(nz) if hop_of(i, nz) in NEAR]


def plain_chunks(nz):
    return [(2 * p, 2) for p in range(nz // 2)]


def slot_entries(nz):
    near = near_positions(nz)
    kinds = [range(NTP) if i in near else (0, 2) if hop_of(i, nz) in TWO else (0,) for i in range(nz)]
    return [(i, q) for i in range(nz) for q in kinds[i]]


def plain_messages(far, two, near):
    return [(i, 0) for i in far] + [(i, 2) for i in two] + [(i, 0) for i in near if i > 0]


def plain_order(messages, far, two, nz):
    steps = [f"Z{k}" for k in range(len(messages))] + [f"O{i}" for i in far]
    steps += [f"F{i}" for i in far if i not in two]
    steps += [f"I{i}" for i in range(nz)]
    for p in range(nz // 2):
        steps += [f"H{p}", f"A{p}"]
        if p < nz // 2 - 1:
            steps += [f"D{p}", f"B{2 * p}", f"B{2 * p + 1}"]
    return steps


def iota(shape, dim):
    return lax.broadcasted_iota(jnp.int32, shape, dim)


def one_hot(hit):
    return jnp.where(hit, 1.0, 0.0).astype(BF16)


def dot_nt(a, b):
    return lax.dot_general(a, b, (((1,), (1,)), ((), ())), preferred_element_type=F32)


def step_kernel(
    nz, nyc, q_hbm, kt_hbm, vt_hbm, sink, ow_hbm, tok_hbm, gain_hbm, rgt_hbm, rex_hbm, rt_hbm,
    wg_hbm, wu_hbm, wd_hbm, mix_hbm, moe,
    gain, rgt, rex, rt, mix,
    tok, normed, comp, meta, order, cin, cin_e, min_, mcol, relay, arr, wg, wu, wq, act,
    out, back, pout, rtok, att, ow, fin_out, fin, qs, kvt, wide,
    zs, zr, ms, mr, ys, yr, yes, yer, xs, xr, fs, fr, acs, acr, afs, afr, ws, wr,
    rzs, rzr, rys, ryr, ts, tr, tfs, tfr, es, er, hs, hr, loc,
):
    x = lax.axis_index("tp")
    e = lax.axis_index("ep")
    z, yc = lax.div(e, nyc), lax.rem(e, nyc)
    fq = arr.shape[-1]
    hq = wg.shape[-1]
    hops = [hop_of(i, nz) for i in range(nz)]
    near = near_positions(nz)
    half = nyc // 2
    chunks = CHUNKS if nz == 8 else plain_chunks(nz)
    tokens, width = tok.shape
    block_rows = tokens // NTP
    rest = pl.ds(1, nyc - 1)

    def zdev(d):
        return (lax.rem(z + (d + nz), nz) * nyc + yc, x)

    def ydev(j):
        return (z * nyc + lax.rem(yc + (j + nyc), nyc), x)

    def xdev(q):
        return (e, lax.rem(x + q, NTP))

    def edev(step):
        return (lax.rem(e + (step + nz * nyc), nz * nyc), x)

    def column(q):
        return lax.rem(x + (q + NTP), NTP)

    def send(src, dst, s_sem, r_sem, dev):
        copy = pltpu.make_async_remote_copy(
            src_ref=src, dst_ref=dst, send_sem=s_sem, recv_sem=r_sem,
            device_id=dev, device_id_type=MESH,
        )
        copy.start()

    def drain(ref, sem):
        pltpu.make_async_copy(ref, ref, sem).wait()

    def quarter(q, size):
        return pl.ds(pl.multiple_of(column(q) * size, size), size)

    barrier = pltpu.get_barrier_semaphore()
    peers = [xdev(q) for q in range(1, NTP)] + [edev(1), edev(-1)]
    peers += [ydev(j) for j in range(1, nyc)] + [zdev(d) for d in range(1, nz)]
    for peer in peers:
        pl.semaphore_signal(barrier, inc=1, device_id=peer, device_id_type=MESH)
    span = kt_hbm.shape[1]
    step = tokens // 4
    local = [
        pltpu.make_async_copy(wg_hbm, wg, loc.at[0]),
        pltpu.make_async_copy(wu_hbm, wu, loc.at[1]),
        pltpu.make_async_copy(wd_hbm.at[:, :, quarter(0, fq)], wq.at[0], loc.at[2]),
        pltpu.make_async_copy(ow_hbm, ow, loc.at[3]),
        pltpu.make_async_copy(q_hbm, qs, loc.at[4]),
        pltpu.make_async_copy(kt_hbm, kvt.at[0, :, pl.ds(WINDOW, span)], loc.at[5]),
        pltpu.make_async_copy(vt_hbm, kvt.at[1, :, pl.ds(WINDOW, span)], loc.at[6]),
    ]
    token_parts = [
        pltpu.make_async_copy(tok_hbm.at[pl.ds(i * step, step)], tok.at[pl.ds(i * step, step)], loc.at[7 + i])
        for i in range(4)
    ]
    small = [
        pltpu.make_async_copy(source, target, loc.at[11 + n])
        for n, (source, target) in enumerate(
            ((gain_hbm, gain), (rt_hbm, rt), (rgt_hbm, rgt), (rex_hbm, rex))
        )
    ]
    for copy in token_parts + small + local:
        copy.start()
    pl.semaphore_wait(barrier, len(peers))

    for q in (1, 3, 2):
        send(wd_hbm.at[:, :, quarter(q, fq)], wq.at[q], ws.at[q], wr.at[q], xdev(q))
    tail = pl.ds(span - WINDOW, WINDOW)
    for w, source in enumerate((kt_hbm, vt_hbm)):
        send(source.at[:, tail], kvt.at[w, :, pl.ds(0, WINDOW)], hs.at[w], hr.at[w], edev(1))

    for copy in small:
        copy.wait()
    for i in range(4):
        token_parts[i].wait()

        def norm_rows(c, carry, i=i):
            where = pl.ds(pl.multiple_of(i * step + c * (step // 2), step // 2), step // 2)
            v = tok[where, :].astype(F32)
            ms = jnp.mean(v * v, axis=-1, keepdims=True)
            normed[where, :] = (v * lax.rsqrt(ms + 1e-06) * gain[...]).astype(BF16)
            return carry

        lax.fori_loop(0, 2, norm_rows, 0)

    experts = rex.shape[1]
    shift = block_rows.bit_length() - 1
    per_group = block_rows // GROUPS
    group_rows = tokens // GROUPS
    planes = nz // GROUPS
    part = nyc * 2 * NTP * CAP
    e0, e1 = rt[0:1, :], rt[1:2, :]
    ids = iota((experts, tokens), 0)
    hit0, hit1 = ids == e0, ids == e1
    first, second = iota((tokens, tokens), 0), iota((tokens, tokens), 1)
    before = one_hot(((first >> shift) == (second >> shift)) & (first < second))
    count = jnp.dot(one_hot(hit0 | hit1), before, preferred_element_type=F32)
    place0 = jnp.sum(jnp.where(hit0, count, 0.0), axis=0, keepdims=True).astype(jnp.int32)
    place1 = jnp.sum(jnp.where(hit1, count, 0.0), axis=0, keepdims=True).astype(jnp.int32)
    group = e0 >> ((experts // GROUPS).bit_length() - 1)
    mine = iota((16, tokens), 0) == group
    count = jnp.dot(one_hot(mine), before, preferred_element_type=F32)
    nth = jnp.sum(jnp.where(mine, count, 0.0), axis=0, keepdims=True).astype(jnp.int32)
    block = iota((1, tokens), 1) >> shift
    in_block = group * per_group + nth
    place = group * group_rows + block * per_group + nth

    def compact(c, carry):
        where = pl.ds(pl.multiple_of(c * group_rows, group_rows), group_rows)
        pick = one_hot(iota((group_rows, tokens), 0) + c * group_rows == place)
        comp[where, :] = jnp.dot(pick, normed[...], preferred_element_type=F32).astype(BF16)
        return carry

    lax.fori_loop(0, GROUPS, compact, 0)

    def group_at(d):
        g = lax.div(lax.rem(z + (d + nz), nz), planes)
        return pl.ds(pl.multiple_of(g * group_rows, group_rows), group_rows)

    far = [i for i in range(nz) if i not in near]
    two = [i for i in far if hops[i] in TWO]
    messages = MESSAGES if nz == 8 else plain_messages(far, two, near)
    entries = slot_entries(nz)

    def plane_send(k):
        i, q = messages[k]
        if i in near:
            source, target = comp.at[group_at(hops[i]), :], cin_e.at[near.index(i)]
        else:
            source, target = comp.at[group_at(hops[i]), quarter(-q, fq)], cin.at[i, q // 2]
        send(source, target, zs.at[k], zr.at[k], zdev(hops[i]))

    for k in range(min(AHEAD, len(messages))):
        plane_send(k)

    by_expert = lax.dot_general(
        rex[...], normed[...], (((0,), (1,)), ((), ())), preferred_element_type=F32
    )
    by_group = dot_nt(rgt[...], normed[...])
    groups = rgt.shape[0]
    group_exp = jnp.exp(by_group - jnp.max(by_group, axis=0, keepdims=True))
    chosen = iota((groups, tokens), 0) == group
    share = jnp.sum(jnp.where(chosen, group_exp, 0.0), axis=0, keepdims=True) / jnp.sum(
        group_exp, axis=0, keepdims=True
    )
    l0 = jnp.sum(jnp.where(hit0, by_expert, 0.0), axis=0, keepdims=True)
    l1 = jnp.sum(jnp.where(hit1, by_expert, 0.0), axis=0, keepdims=True)
    top = jnp.maximum(l0, l1)
    x0, x1 = jnp.exp(l0 - top), jnp.exp(l1 - top)

    def plane_row(expert, place):
        j = (((expert >> 1) & (nyc - 1)) - yc + nyc) & (nyc - 1)
        return (j * 2 + (expert & 1)) * (NTP * CAP) + block * CAP + place

    def plane_of(expert):
        return expert >> nyc.bit_length()

    def pieces(value):
        high = value.astype(BF16).astype(F32)
        middle = (value - high).astype(BF16).astype(F32)
        return (high, middle, value - high - middle)

    values = [plane_row(e0, place0), plane_row(e1, place1), plane_of(e0), plane_of(e1)]
    values += [*pieces(share * (x0 / (x0 + x1))), *pieces(share * (x1 / (x0 + x1)))]
    lanes = iota((16, tokens), 0)
    table = jnp.zeros((16, tokens), F32)
    for at, value in enumerate(values):
        table = jnp.where(lanes == at, value.astype(F32), table)
    spread = one_hot(first == place)
    turned = dot_nt(table.astype(BF16), spread)
    for g in range(GROUPS):
        meta[g] = turned[:, g * group_rows : (g + 1) * group_rows]
    order[...] = jnp.broadcast_to(in_block.astype(F32), order.shape)
    for i in range(1, nz):
        g = lax.div(lax.rem(z + (hops[i] + nz), nz), planes)
        send(meta.at[g], min_.at[i], ms.at[i], mr.at[i], zdev(hops[i]))
    min_[0] = meta[lax.div(z, planes)]

    eye = one_hot(iota((group_rows, group_rows), 0) == iota((group_rows, group_rows), 1))

    def plane_out(k):
        i, first_q = (0, 0) if k < 0 else messages[k]
        if i > 0:
            drain(cin_e.at[near.index(i)] if i in near else cin.at[i, first_q // 2], zr.at[k])
            for following in range(k + AHEAD + (k > WIDEN), k + AHEAD + 1 + (k >= WIDEN)):
                if following < len(messages):
                    plane_send(following)
            if first_q == 0:
                drain(min_.at[i], mr.at[i])
        given = min_[i]
        if first_q == 0:
            mcol[i] = dot_nt(eye, given.astype(BF16))
        row0 = jnp.where(given[2:3, :].astype(jnp.int32) == z, given[0:1, :].astype(jnp.int32), -1)
        row1 = jnp.where(given[3:4, :].astype(jnp.int32) == z, given[1:2, :].astype(jnp.int32), -1)
        ids = iota((part, group_rows), 0)
        pick = one_hot((ids == row0) | (ids == row1))
        for q in range(NTP) if i in near else (first_q,):
            if i == 0:
                rows = comp[group_at(0), quarter(-q, fq)]
            elif i in near:
                rows = cin_e[near.index(i), :, quarter(-q, fq)]
            else:
                rows = cin[i, q // 2]
            got = jnp.dot(pick, rows, preferred_element_type=F32).astype(BF16)
            got = got.reshape(nyc, 2, NTP * CAP, fq)
            at = entries.index((i, q))
            arr[q, i, 0] = got[0]
            relay[at, rest] = got[1:]
            for j in range(1, nyc):
                if q == 0:
                    send(relay.at[at, j], arr.at[0, i, j], ys.at[i], yr.at[i], ydev(j))
                else:
                    send(relay.at[at, j], arr.at[q, i, j], yes.at[i], yer.at[i], ydev(j))

    def others(i):
        if i in near:
            return arr.at[pl.ds(1, NTP - 1), i, rest]
        return arr.at[2, i, rest]

    heads = qs.shape[1] // HD
    for copy in local[4:7]:
        copy.wait()
    for w in range(2):
        drain(kvt.at[w, :, pl.ds(0, WINDOW)], hr.at[w])
    for w in range(2):
        for h in range(heads):
            for other in range(heads):
                if other != h:
                    wide[w, h, pl.ds(other * HD, HD), :] = jnp.zeros((HD, span + WINDOW), BF16)
            wide[w, h, pl.ds(h * HD, HD), :] = kvt[w]

    def attend(b, carry):
        where = pl.ds(pl.multiple_of(b * WINDOW, WINDOW), WINDOW)
        band = pl.ds(pl.multiple_of(b * WINDOW, WINDOW), 2 * WINDOW)
        key = iota((WINDOW, 2 * WINDOW), 1)
        distance = iota((WINDOW, 2 * WINDOW), 0) + WINDOW - key
        earliest = jnp.where(e + b == 0, WINDOW, 0)
        allowed = (distance >= 0) & (distance < WINDOW) & (key >= earliest)
        queries = qs[where, :]
        total = jnp.zeros((WINDOW, heads * HD), F32)
        for h in range(heads):
            scores = jnp.dot(queries, wide[0, h, :, band], preferred_element_type=F32)
            masked = jnp.where(allowed, scores * HD ** (-0.5), -1e30)
            row_max = jnp.maximum(jnp.max(masked, axis=1, keepdims=True), sink[h])
            weights = jnp.exp(masked - row_max)
            denominator = jnp.sum(weights, axis=1, keepdims=True) + jnp.exp(sink[h] - row_max)
            probs = (weights / denominator).astype(BF16)
            total += dot_nt(probs, wide[1, h, :, band])
        att[0, where, :] = total.astype(BF16)
        return carry

    lax.fori_loop(0, span // WINDOW, attend, 0)

    def ring_own(i):
        drain(arr.at[0, i, rest], yr.at[i])
        send(arr.at[0, i], arr.at[1, i], xs.at[i, 0], xr.at[i, 0], xdev(1))
        send(arr.at[0, i], arr.at[3, i], xs.at[i, 1], xr.at[i, 1], xdev(3))

    low, high = pl.ds(0, half), pl.ds(half, half)

    def ring_on(i):
        drain(arr.at[1, i], xr.at[i, 0])
        send(arr.at[1, i, low], arr.at[2, i, low], fs.at[i, 0], fr.at[i, 0], xdev(1))
        drain(arr.at[3, i], xr.at[i, 1])
        send(arr.at[3, i, high], arr.at[2, i, high], fs.at[i, 1], fr.at[i, 1], xdev(3))

    def ring_in(i):
        if i in near:
            drain(arr.at[0, i, rest], yr.at[i])
        elif i in two:
            drain(arr.at[1, i], xr.at[i, 0])
            drain(arr.at[3, i], xr.at[i, 1])
        else:
            drain(arr.at[2, i, low], fr.at[i, 0])
            drain(arr.at[2, i, high], fr.at[i, 1])
            return
        drain(others(i), yer.at[i])

    rows1 = nyc * NTP * CAP

    def span_of(c):
        first, many = chunks[c]
        return pl.ds(first, many), many * rows1

    def hidden(c):
        if c == 0:
            local[0].wait()
            local[1].wait()
        span, rows2 = span_of(c)

        def one(k, carry):
            gate = jnp.zeros((rows2, hq), F32)
            up = jnp.zeros((rows2, hq), F32)
            for q in range(NTP):
                depth = quarter(-q, fq)
                rows = arr[q, span, :, k].reshape(rows2, fq)
                gate += jnp.dot(rows, wg[k, depth, :], preferred_element_type=F32)
                up += jnp.dot(rows, wu[k, depth, :], preferred_element_type=F32)
            value = (gate / (1.0 + jnp.exp(-gate)) * up).astype(BF16)
            act[0, span, k] = value.reshape(-1, rows1, hq)
            return carry

        lax.fori_loop(0, 2, one, 0)
        send(act.at[0, span], act.at[1, span], acs.at[c, 0], acr.at[c, 0], xdev(1))
        send(act.at[0, span], act.at[3, span], acs.at[c, 1], acr.at[c, 1], xdev(3))

    def act_on(c):
        span, _ = span_of(c)
        drain(act.at[1, span], acr.at[c, 0])
        send(act.at[1, span, 0], act.at[2, span, 0], afs.at[c, 0], afr.at[c, 0], xdev(1))
        drain(act.at[3, span], acr.at[c, 1])
        send(act.at[3, span, 1], act.at[2, span, 1], afs.at[c, 1], afr.at[c, 1], xdev(3))

    def down(c):
        if c == 0:
            local[2].wait()
            for q in range(1, NTP):
                drain(wq.at[q], wr.at[q])
        span, rows2 = span_of(c)
        drain(act.at[2, span, 0], afr.at[c, 0])
        drain(act.at[2, span, 1], afr.at[c, 1])

        def one(k, carry):
            total = jnp.zeros((rows2, fq), F32)
            for q in range(NTP):
                rows = act[q, span, k].reshape(rows2, hq)
                total += jnp.dot(rows, wq[q, k], preferred_element_type=F32)
            out[span, :, k] = total.astype(BF16).reshape(-1, nyc, NTP * CAP, fq)
            return carry

        lax.fori_loop(0, 2, one, 0)
        for i in range(chunks[c][0], sum(chunks[c])):
            for j in range(1, nyc):
                send(out.at[i, j], back.at[i, j], rys.at[i], ryr.at[i], ydev(-j))
            back[i, 0] = out[i, 0]

    def plane_back(i):
        drain(back.at[i, rest], ryr.at[i])
        given = mcol[i]
        ids = iota((group_rows, part), 1)
        picks = []
        for k in range(2):
            row = given[:, k : k + 1].astype(jnp.int32)
            here = given[:, 2 + k : 3 + k].astype(jnp.int32) == z
            picks.append(one_hot(ids == jnp.where(here, row, -1)))
        got = jnp.dot(
            jnp.concatenate(picks, axis=0), back[i].reshape(part, fq), preferred_element_type=F32
        )
        g0 = given[:, 4:5] + given[:, 5:6] + given[:, 6:7]
        g1 = given[:, 7:8] + given[:, 8:9] + given[:, 9:10]
        total = (g0 * got[:group_rows] + g1 * got[group_rows:]).astype(BF16)
        if i == 0:
            rtok[0] = total
            return
        pout[i] = total
        send(pout.at[i], rtok.at[hops[i]], rzs.at[i], rzr.at[i], zdev(-hops[i]))

    rows = att.shape[1]
    top_half, low_half = pl.ds(0, rows // 2), pl.ds(rows // 2, rows // 2)

    def heads_ring(part):
        if part == 0:
            send(att.at[0], att.at[1], ts.at[0], tr.at[0], xdev(1))
            send(att.at[0], att.at[3], ts.at[1], tr.at[1], xdev(3))
            return
        drain(att.at[1], tr.at[0])
        send(att.at[1, top_half], att.at[2, top_half], tfs.at[0], tfr.at[0], xdev(1))
        drain(att.at[3], tr.at[1])
        send(att.at[3, low_half], att.at[2, low_half], tfs.at[1], tfr.at[1], xdev(3))

    steps = {
        "Z": plane_out, "O": ring_own, "F": ring_on, "I": ring_in, "H": hidden,
        "A": act_on, "D": down, "B": plane_back, "T": heads_ring,
    }
    for step in MIDDLE if nz == 8 else plain_order(messages, far, two, nz):
        steps[step[0]](int(step[1:]))
    for step in TAIL if nz == 8 else ("T0", f"D{len(chunks) - 1}", f"B{nz - 2}", f"B{nz - 1}", "T1"):
        steps[step[0]](int(step[1:]))
    local[3].wait()
    chunk = rows // 4
    hw = att.shape[2]

    def project(c, carry):
        where = pl.ds(pl.multiple_of(c * chunk, chunk), chunk)
        total = jnp.zeros((chunk, ow.shape[1]), F32)
        for q in range(NTP):
            total += jnp.dot(att[q, where, :], ow[quarter(-q, hw), :], preferred_element_type=F32)
        mix[where, :] = total.astype(BF16)
        return carry

    for i in range(1, nz):
        drain(rtok.at[hops[i]], rzr.at[i])

    def combined(t):
        where = pl.ds(pl.multiple_of(t * per_group, per_group), per_group)
        found = []
        for g in range(GROUPS):
            total = jnp.zeros((per_group, fq), F32)
            for p in range(planes):
                d = lax.rem(g * planes + p + nz - z, nz)
                total += rtok[d, where, :].astype(F32)
            found.append(total.astype(BF16))
        return jnp.concatenate(found, axis=0)

    for q in (2, 1, 3):
        fin_out[q] = combined(column(q))
        send(fin_out.at[q], fin.at[q], es.at[q], er.at[q], xdev(q))
    drain(att.at[2, top_half], tfr.at[0])
    drain(att.at[2, low_half], tfr.at[1])
    lax.fori_loop(0, 4, project, 0)
    mixed = pltpu.make_async_copy(mix, mix_hbm, loc.at[15])
    mixed.start()
    own = combined(x)
    turned = order[:, pl.ds(pl.multiple_of(x * block_rows, block_rows), block_rows)]
    rows, cols = iota((block_rows, block_rows), 0), iota((block_rows, block_rows), 1)
    turned = dot_nt(one_hot(rows == cols), turned.astype(BF16)).astype(jnp.int32)
    spread = one_hot(cols == turned[:, 0:1])
    moe[:, quarter(0, fq)] = jnp.dot(spread, own, preferred_element_type=F32).astype(BF16)
    for q in (1, 3, 2):
        drain(fin.at[q], er.at[q])
        placed = jnp.dot(spread, fin[q], preferred_element_type=F32).astype(BF16)
        moe[:, quarter(-q, fq)] = placed

    mixed.wait()
    for k, (i, q) in enumerate(messages):
        drain(cin_e.at[near.index(i)] if i in near else cin.at[i, q // 2], zs.at[k])
    for i in range(nz):
        drain(arr.at[0, i, rest], ys.at[i])
        if i in near or i in two:
            drain(others(i), yes.at[i])
        drain(back.at[i, rest], rys.at[i])
        if i > 0:
            drain(min_.at[i], ms.at[i])
            drain(pout.at[i], rzs.at[i])
        if i in near:
            continue
        for way in range(2):
            drain(arr.at[0, i], xs.at[i, way])
            if i not in two:
                drain(arr.at[0, i, low], fs.at[i, way])
    for c in range(len(chunks)):
        span, _ = span_of(c)
        for way in range(2):
            drain(act.at[0, span], acs.at[c, way])
            drain(act.at[0, span, 0], afs.at[c, way])
    for way in range(2):
        drain(att.at[0], ts.at[way])
        drain(att.at[0, top_half], tfs.at[way])
        drain(kvt.at[way, :, pl.ds(0, WINDOW)], hs.at[way])
    for q in range(1, NTP):
        drain(wq.at[q], ws.at[q])
        drain(fin_out.at[q], es.at[q])


def per_device(
    q_heads,
    k_heads,
    v_heads,
    sink_logits,
    out_weight,
    tokens_b,
    moe_gain,
    router_group,
    router_expert,
    route_expert,
    expert_gate,
    expert_up,
    expert_down,
):
    nyc = min(PLANE, lax.axis_size("ep"))
    nz = lax.axis_size("ep") // nyc
    tokens, width = tokens_b.shape
    fq = width // NTP
    hq = expert_gate.shape[2]
    sixteen = NTP * CAP
    span = q_heads.shape[0]
    vmem = pl.BlockSpec(memory_space=pltpu.VMEM)
    smem = pl.BlockSpec(memory_space=pltpu.SMEM)
    anywhere = pl.BlockSpec(memory_space=pl.ANY)
    dma = pltpu.SemaphoreType.DMA
    chunks = len(CHUNKS if nz == 8 else plain_chunks(nz))
    near = len(near_positions(nz))
    slot = (nz, nyc, 2, sixteen, fq)
    group_rows = tokens // GROUPS
    return pl.pallas_call(
        functools.partial(step_kernel, nz, nyc),
        out_shape=(
            jax.ShapeDtypeStruct((span, out_weight.shape[1]), BF16),
            jax.ShapeDtypeStruct((tokens // NTP, width), BF16),
        ),
        in_specs=[anywhere] * 3 + [smem] + [anywhere] * 9,
        out_specs=(anywhere, vmem),
        scratch_shapes=[
            pltpu.VMEM((1, width), F32),
            pltpu.VMEM((router_group.shape[1], width), BF16),
            pltpu.VMEM(router_expert.shape, BF16),
            pltpu.VMEM((2, tokens), jnp.int32),
            pltpu.VMEM((span, out_weight.shape[1]), BF16),
            pltpu.VMEM(tokens_b.shape, BF16),
            pltpu.VMEM(tokens_b.shape, BF16),
            pltpu.VMEM(tokens_b.shape, BF16),
            pltpu.VMEM((GROUPS, 16, group_rows), F32),
            pltpu.VMEM((8, tokens), F32),
            pltpu.VMEM((nz, 2, group_rows, fq), BF16),
            pltpu.VMEM((near, group_rows, width), BF16),
            pltpu.VMEM((nz, 16, group_rows), F32),
            pltpu.VMEM((nz, group_rows, 16), F32),
            pltpu.VMEM((len(slot_entries(nz)), *slot[1:]), BF16),
            pltpu.VMEM((NTP, *slot), BF16),
            pltpu.VMEM(expert_gate.shape, BF16),
            pltpu.VMEM(expert_up.shape, BF16),
            pltpu.VMEM((NTP, 2, hq, fq), BF16),
            pltpu.VMEM((NTP, nz, 2, nyc * sixteen, hq), BF16),
            pltpu.VMEM(slot, BF16),
            pltpu.VMEM(slot, BF16),
            pltpu.VMEM((nz, group_rows, fq), BF16),
            pltpu.VMEM((nz, group_rows, fq), BF16),
            pltpu.VMEM((NTP, *q_heads.shape), BF16),
            pltpu.VMEM(out_weight.shape, BF16),
            pltpu.VMEM((NTP, tokens // NTP, fq), BF16),
            pltpu.VMEM((NTP, tokens // NTP, fq), BF16),
            pltpu.VMEM(q_heads.shape, BF16),
            pltpu.VMEM((2, HD, span + WINDOW), BF16),
            pltpu.VMEM((2, q_heads.shape[1] // HD, q_heads.shape[1], span + WINDOW), BF16),
            dma((2 * nz,)), dma((2 * nz,)), dma((nz,)), dma((nz,)),
            dma((nz,)), dma((nz,)), dma((nz,)), dma((nz,)),
            dma((nz, 2)), dma((nz, 2)), dma((nz, 2)), dma((nz, 2)),
            dma((chunks, 2)), dma((chunks, 2)), dma((chunks, 2)), dma((chunks, 2)),
            dma((NTP,)), dma((NTP,)),
            dma((nz,)), dma((nz,)), dma((nz,)), dma((nz,)),
            dma((2,)), dma((2,)), dma((2,)), dma((2,)),
            dma((NTP,)), dma((NTP,)), dma((2,)), dma((2,)), dma((16,)),
        ],
        compiler_params=pltpu.CompilerParams(
            collective_id=0, has_side_effects=True, vmem_limit_bytes=62 * 2**20
        ),
        name="step",
    )(
        q_heads,
        k_heads.T,
        v_heads.T,
        sink_logits,
        out_weight,
        tokens_b,
        moe_gain.reshape(1, width),
        router_group.T,
        router_expert,
        route_expert.T,
        expert_gate,
        expert_up,
        expert_down,
    )


def solution(mesh):
    in_specs = (
        P("ep", "tp"),
        P("ep", "tp"),
        P("ep", "tp"),
        P("tp"),
        P(None, "tp"),
        P("ep", None),
        P(),
        P(),
        P(),
        P("ep", None),
        P("ep", None, "tp"),
        P("ep", None, "tp"),
        P("ep", "tp", None),
    )
    out_specs = (P("ep", "tp"), P(("ep", "tp"), None))
    return jax.shard_map(
        per_device, mesh=mesh, in_specs=in_specs, out_specs=out_specs, check_vma=False
    )
```
